256 devices in a mesh: ep: 64 (over z, y, core), tp: 4 (over x).
Axes of the slice: x: 4, y: 4, z: 8, core: 2. Of those that a mesh axis runs over, the one named last changes fastest.
Arguments:
- query_rows: bfloat16 [8192, 1024], P('ep', 'tp'), may hold values from -10 to 10
- key_rows: bfloat16 [8192, 1024], P('ep', 'tp'), may hold values from -10 to 10
- value_rows: bfloat16 [8192, 1024], P('ep', 'tp'), may hold values from -6 to 6
- key_bias: bfloat16 [8192, 16], P('ep', 'tp'), may hold values from -24 to 4
- mixer_weight: bfloat16 [1024, 2048], P('tp'), may hold values from -0.1875 to 0.1875
- mixer_gain: float32 [2048], replicated, may hold values from 0.1 to 1.9
- routed_input: bfloat16 [24576, 2048], P(('ep', 'tp')), may hold values from -6 to 6
- entry_gain: float32 [2048], replicated, may hold values from 0.1 to 1.9
- expert_index: int32 [24576, 2], P(('ep', 'tp')), may hold values from 0 to 127, all different within a row; in each aligned block of 96 rows (0 to 95, 96 to 191, ...) at most 2 rows name the same one
- route_weights: float32 [24576, 2], P(('ep', 'tp')), may hold values from 0.1 to 1
- expert_gate: bfloat16 [128, 2048, 1024], P('ep', None, 'tp'), may hold values from -0.125 to 0.125
- expert_up: bfloat16 [128, 2048, 1024], P('ep', None, 'tp'), may hold values from -0.125 to 0.125
- expert_down: bfloat16 [128, 1024, 2048], P('ep', 'tp'), may hold values from -0.1875 to 0.1875
- shared_gate: bfloat16 [2048, 1024], P(None, 'tp'), may hold values from -0.125 to 0.125
- shared_up: bfloat16 [2048, 1024], P(None, 'tp'), may hold values from -0.125 to 0.125
- shared_down: bfloat16 [1024, 2048], P('tp'), may hold values from -0.1875 to 0.1875
- exit_gain: float32 [2048], replicated, may hold values from 0.1 to 1.9
Outputs:
- mixer_out: bfloat16 [8192, 2048], P(('ep', 'tp'))
- expert_out: bfloat16 [24576, 2048], P(('ep', 'tp'))
The draws below stay inside these ranges and needn't reach their ends.
Inputs may be any that keep to these rules, and one draw needn't show every extreme that they name: `expert_index`: in each aligned block of 96 rows (the rows of one device) no expert is named by more than 2 rows, a bound that some block reaches; each row names 2 different experts.
All inputs are finite; a program needn't handle non-finite values.
Results may differ from the reference program's by a relative error of at most 0.012.
Values may be sent and summed in bfloat16 or wider, within the bound.
A program may use at most 128 MiB of HBM per device.

```python
import math
import jax
import jax.numpy as jnp
import numpy as np
from jax import lax

D = 2048
HEADS = 16
HEAD_DIM = 64
FF = 1024
FF_SH = 1024
TOPK = 2
TOK_A = 128
ROWS_B = 96
TOKENS_A = 8192
TOKENS_B = 24576
EXPERTS = 128
CAP = 2
N_EP = 64
N_TP = 4


def draw_key_bias(key, part):
    random_subkeys = jax.random.split(key, 7)
    sequence_length = TOKENS_A
    head_count = HEADS
    head_draw = jax.random.uniform(random_subkeys[0], (head_count,))
    quick_heads = (head_draw < 0.5) | (head_draw <= jnp.min(head_draw))
    keep_share = jax.random.uniform(random_subkeys[1], (head_count,), minval=0.4, maxval=1.2)
    fast_reach = jax.random.uniform(random_subkeys[2], (head_count,), minval=30.0, maxval=50.0)
    noise_shift = 3.3
    slow_level = jnp.log(keep_share / sequence_length) - noise_shift
    fast_level = -jnp.log(fast_reach) - noise_shift
    base_level = jnp.where(quick_heads, fast_level, slow_level)
    shard_count = sequence_length // TOK_A
    shard_shift = jax.random.uniform(random_subkeys[3], (shard_count, head_count), minval=-0.7, maxval=0.7)
    shard_shift = jnp.repeat(shard_shift, TOK_A, axis=0)
    roughness = 0.3 * jax.random.normal(random_subkeys[4], (sequence_length, head_count))
    logarithm_bias = base_level[None, :] + shard_shift + roughness
    spike_positions = jax.random.randint(random_subkeys[5], (3,), 0, sequence_length)
    spike_rows = jnp.any(jnp.arange(sequence_length)[:, None] == spike_positions[None, :], axis=1)
    remaining_fraction = jax.random.uniform(random_subkeys[6], (sequence_length, head_count), minval=0.2, maxval=0.5)
    spike_level = jnp.log(remaining_fraction / (1.0 - remaining_fraction))
    logarithm_bias = jnp.where(spike_rows[:, None] & (~quick_heads)[None, :], spike_level, logarithm_bias)
    return logarithm_bias.astype(jnp.float32).astype(jnp.bfloat16)


def block_levels(key, dims, cuts, low, largest):
    level, own = 1.0, jax.random.fold_in(key, 6)
    for axis_at, blocks in cuts:
        heights = jnp.exp(jax.random.uniform(jax.random.fold_in(own, axis_at), (blocks,), jnp.float32, low / len(cuts), largest / len(cuts)))
        level = level * jnp.repeat(heights, dims[axis_at] // blocks).reshape([-1 if axis == axis_at else 1 for axis in range(len(dims))])
    return level


def deal_out(own_key, own, number, rows, number_of, top, reach, skew):
    ranking = jax.random.permutation(own_key, number_of)
    heavy_load, common = shares(number_of, rows * top, reach, skew, True), shares(number_of, rows * top, reach, skew, False)
    places = jnp.arange(number_of)

    def named(tallies, offset_by):
        used = int((tallies > 0).sum())
        fixed = max(1, used // 4)
        moved = fixed + (places - fixed + offset_by * (used - fixed)) % max(1, number_of - fixed)
        return jnp.zeros((number_of,), jnp.int32).at[ranking[jnp.where(places < fixed, places, moved)]].set(jnp.asarray(tallies, jnp.int32))

    tallies = jnp.where(number % 4 == 0, named(heavy_load, number // 4), named(common, number - number // 4 - 1))
    mixed = jax.random.permutation(jax.random.fold_in(own, 3), number_of)
    source_of, receiver = mixed[0:number_of // 2 * 2:2], mixed[1:number_of // 2 * 2:2]
    margin = jnp.minimum(tallies[source_of] - 1, reach - tallies[receiver]) // 2
    margin = jnp.where((source_of == ranking[0]) | (receiver == ranking[0]) | (tallies[receiver] == 0), 0, jnp.maximum(margin, 0))
    moved = jax.random.randint(jax.random.fold_in(own, 4), (number_of // 2,), 0, 1 << 20) % (margin + 1)
    tallies = tallies.at[source_of].add(-moved).at[receiver].add(moved)
    labels = jnp.searchsorted(jnp.cumsum(tallies), jnp.arange(rows * top), side="right").astype(jnp.int32)
    listing = labels.reshape(top, rows).T
    listing = listing[jax.random.permutation(jax.random.fold_in(own, 1), rows)]
    offset_by = jax.random.randint(jax.random.fold_in(own, 2), (rows, 1), 0, top)
    return jnp.take_along_axis(listing, (jnp.arange(top)[None, :] + offset_by) % top, axis=1)


def shares(count, total, bound, slope, full):
    loads = [(1 << 20) // math.isqrt(grade ** slope) + 1 for grade in range(1, count + 1)]
    largest = bound if full else min(bound, max(-(-total // count), total * loads[0] // sum(loads)))
    least = 1 if total - largest >= count - 1 else 0
    holding, surplus = [largest] + [least] * (count - 1), total - largest - least * (count - 1)
    while surplus > 0:
        movable = [i for i in range(1, count) if holding[i] < largest] or [i for i in range(1, count) if holding[i] < bound]
        whole, left = sum([loads[i] for i in movable]), surplus
        for i in movable:
            addition = min(bound - holding[i], max(1, left * loads[i] // whole), surplus)
            holding[i] = holding[i] + addition
            surplus = surplus - addition
    return np.array(holding)


def gaussian(rng, shape, deviation, bound, cuts=(), kind=jnp.bfloat16):
    array = jax.random.normal(rng, shape, jnp.float32) * deviation
    if len(cuts) > 0:
        array = block_levels(rng, shape, cuts, -0.22, 0.18) * array
    return jnp.clip(array, min=-bound, max=bound).astype(kind)


def setup_inputs(seed: int = 0) -> dict:
    seeds = jax.random.split(jax.random.key(seed), 18)
    query_rows = gaussian(seeds[0], (TOKENS_A, HEADS * HEAD_DIM), 1.6, 10.0, ((0, 64), (1, 4)))
    key_rows = gaussian(seeds[1], (TOKENS_A, HEADS * HEAD_DIM), 1.6, 10.0, ((0, 64), (1, 4)))
    value_rows = gaussian(seeds[2], (TOKENS_A, HEADS * HEAD_DIM), 1.0, 6.0, ((0, 64), (1, 4)))
    key_bias = draw_key_bias(jax.random.fold_in(seeds[17], 71), 0)
    mixer_weight = gaussian(seeds[4], (HEADS * HEAD_DIM, D), (HEADS * HEAD_DIM) ** -0.5, 0.1875, ((0, 4),))
    mixer_gain = jnp.clip(1.0 + 0.18 * jax.random.normal(seeds[5], (D,), jnp.float32), 0.1, 1.9)
    routed_input = gaussian(seeds[6], (TOKENS_B, D), 1.0, 6.0, ((0, 256),))
    entry_gain = jnp.clip(1.0 + 0.18 * jax.random.normal(seeds[7], (D,), jnp.float32), 0.1, 1.9)
    expert_index_keys = jax.random.split(jax.random.fold_in(seeds[8], 1), TOKENS_B // ROWS_B)
    expert_index_turns = jax.random.permutation(jax.random.fold_in(seeds[8], 3), TOKENS_B // ROWS_B)
    expert_index = jax.vmap(lambda own, number: deal_out(jax.random.fold_in(seeds[8], 2), own, number, ROWS_B, EXPERTS, TOPK, CAP, 2))(expert_index_keys, expert_index_turns).reshape((TOKENS_B, TOPK))
    route_weights = jnp.clip(jnp.exp(math.log(1.0) - 2.3025851 * jax.random.uniform(seeds[9], (TOKENS_B, TOPK), jnp.float32) ** block_levels(seeds[9], (TOKENS_B, TOPK), ((0, 256),), -0.2, 0.2)), 0.1, 1.0)
    expert_gate = gaussian(seeds[10], (EXPERTS, D, FF), D ** -0.5, 0.125, ((0, 64), (2, 4)))
    expert_up = gaussian(seeds[11], (EXPERTS, D, FF), D ** -0.5, 0.125, ((0, 64), (2, 4)))
    expert_down = gaussian(seeds[12], (EXPERTS, FF, D), FF ** -0.5, 0.1875, ((0, 64), (1, 4)))
    shared_gate = gaussian(seeds[13], (D, FF_SH), D ** -0.5, 0.125, ((1, 4),))
    shared_up = gaussian(seeds[14], (D, FF_SH), D ** -0.5, 0.125, ((1, 4),))
    shared_down = gaussian(seeds[15], (FF_SH, D), FF_SH ** -0.5, 0.1875, ((0, 4),))
    exit_gain = jnp.clip(1.0 + 0.18 * jax.random.normal(seeds[16], (D,), jnp.float32), 0.1, 1.9)
    return dict(query_rows=query_rows, key_rows=key_rows, value_rows=value_rows, key_bias=key_bias, mixer_weight=mixer_weight, mixer_gain=mixer_gain, routed_input=routed_input, entry_gain=entry_gain, expert_index=expert_index, route_weights=route_weights, expert_gate=expert_gate, expert_up=expert_up, expert_down=expert_down, shared_gate=shared_gate, shared_up=shared_up, shared_down=shared_down, exit_gain=exit_gain)


EPS = 1e-06

def root_norm(values, gain_row):
    return values * lax.rsqrt(lax.optimization_barrier(jnp.mean(values * values, axis=-1, keepdims=True)) + EPS) * gain_row

def key_shards():
    shards = 1
    while shards * TOK_A < 512 and N_EP % (2 * shards) == 0:
        shards = shards * 2
    return shards

def stick_breaking(query_rows, key_rows, value_rows, key_bias):
    total_rows = query_rows.shape[0]
    block_rows = key_shards() * TOK_A
    query_split = query_rows.reshape(N_EP, TOK_A, HEADS, HEAD_DIM).astype(jnp.float32)
    keys_split = key_rows.reshape(total_rows, HEADS, HEAD_DIM).astype(jnp.float32)
    values_split = value_rows.reshape(total_rows, HEADS, HEAD_DIM).astype(jnp.float32)
    bias_split = jnp.transpose(key_bias.astype(jnp.float32))
    score_scale = HEAD_DIM ** (-0.5)

    def one_shard(shard_pair):
        shard_query, shard_index = shard_pair
        query_pos = shard_index * TOK_A + jnp.arange(TOK_A, dtype=jnp.int32)
        own_block = shard_index * TOK_A // block_rows

        def backward_turn(turn_index, carried_pair):
            output, carried = carried_pair
            block_start = ((own_block - turn_index) * block_rows).astype(jnp.int32)
            block_keys = lax.dynamic_slice_in_dim(keys_split, block_start, block_rows, 0)
            block_values = lax.dynamic_slice_in_dim(values_split, block_start, block_rows, 0)
            block_bias = lax.dynamic_slice_in_dim(bias_split, block_start, block_rows, 1)
            scores = jnp.einsum('qhd,khd->hqk', shard_query, block_keys) * score_scale + block_bias[:, None, :]
            key_pos = block_start + jnp.arange(block_rows, dtype=jnp.int32)
            causal = (key_pos[None, :] < query_pos[:, None])[None]
            fail_logs = jnp.where(causal, -jax.nn.softplus(scores), 0.0)
            later_sum = lax.cumsum(fail_logs, axis=2, reverse=True) - fail_logs + carried[:, :, None]
            weights = jnp.where(causal, jnp.exp(jax.nn.log_sigmoid(scores) + later_sum), 0.0)
            weights = lax.optimization_barrier(weights.astype(jnp.bfloat16)).astype(jnp.float32)
            output = output + jnp.einsum('hqk,khd->qhd', weights, block_values)
            return (output, carried + lax.optimization_barrier(jnp.sum(fail_logs, axis=2)))
        zero_output = jnp.zeros((TOK_A, HEADS, HEAD_DIM), jnp.float32)
        zero_carried = jnp.zeros((HEADS, TOK_A), jnp.float32)
        output, unused = lax.fori_loop(0, own_block + 1, backward_turn, (zero_output, zero_carried))
        return output
    outputs = lax.map(one_shard, (query_split, jnp.arange(N_EP, dtype=jnp.int32)))
    return outputs.reshape(total_rows, HEADS * HEAD_DIM).astype(jnp.bfloat16)

def grouped_product(left_rows, right_matrix):
    part_width = left_rows.shape[1] // N_TP
    summed = jnp.zeros((left_rows.shape[0], right_matrix.shape[1]), jnp.float32)
    for part_index in range(N_TP):
        lower = part_index * part_width
        piece_sum = jnp.dot(left_rows[:, lower:lower + part_width], right_matrix[lower:lower + part_width], preferred_element_type=jnp.float32).astype(jnp.bfloat16)
        summed = summed + lax.optimization_barrier(piece_sum).astype(jnp.float32)
    return summed

def swiglu(chosen_rows, gate_weight, up_weight):
    gate_part = jnp.dot(chosen_rows, gate_weight, preferred_element_type=jnp.float32)
    up_part = jnp.dot(chosen_rows, up_weight, preferred_element_type=jnp.float32)
    return (jax.nn.silu(gate_part) * up_part).astype(jnp.bfloat16)

def routed_experts(normed, expert_index, route_weights, expert_gate, expert_up, expert_down):
    token_count = normed.shape[0]
    flat_expert = expert_index.reshape(-1).astype(jnp.int32)
    flat_token = jnp.repeat(jnp.arange(token_count, dtype=jnp.int32), TOPK)
    flat_weight = route_weights.reshape(-1)
    sort_order = jnp.argsort(flat_expert, stable=True)
    window = token_count // ROWS_B * CAP
    sorted_token = jnp.concatenate([flat_token[sort_order], jnp.zeros((window,), jnp.int32)])
    sorted_weight = jnp.concatenate([flat_weight[sort_order], jnp.zeros((window,), flat_weight.dtype)])
    counts = jax.ops.segment_sum(jnp.ones_like(flat_expert), flat_expert, EXPERTS).astype(jnp.int32)
    starts = (jnp.cumsum(counts) - counts).astype(jnp.int32)

    def one_expert(routed, expert_number):
        first_slot = starts[expert_number]
        tokens = lax.dynamic_slice_in_dim(sorted_token, first_slot, window)
        weights = lax.dynamic_slice_in_dim(sorted_weight, first_slot, window)
        live_slots = jnp.arange(window, dtype=jnp.int32) < counts[expert_number]
        chosen_rows = normed[tokens]
        hidden = swiglu(chosen_rows, expert_gate[expert_number], expert_up[expert_number])
        output = grouped_product(hidden, expert_down[expert_number]).astype(jnp.bfloat16)
        output = lax.optimization_barrier(output).astype(jnp.float32)
        return (routed.at[tokens].add(jnp.where(live_slots, weights, 0.0)[:, None] * output), None)
    routed, unused = lax.scan(one_expert, jnp.zeros((token_count, D), jnp.float32), jnp.arange(EXPERTS, dtype=jnp.int32))
    return routed

def reference(query_rows, key_rows, value_rows, key_bias, mixer_weight, mixer_gain, routed_input, entry_gain, expert_index, route_weights, expert_gate, expert_up, expert_down, shared_gate, shared_up, shared_down, exit_gain):
    attended = stick_breaking(query_rows, key_rows, value_rows, key_bias)
    mixer_sum = grouped_product(attended, mixer_weight)
    mixer_out = root_norm(mixer_sum, mixer_gain).astype(jnp.bfloat16)
    normed = root_norm(routed_input.astype(jnp.float32), entry_gain).astype(jnp.bfloat16)
    routed = routed_experts(normed, expert_index, route_weights, expert_gate, expert_up, expert_down)
    shared_hidden = swiglu(normed, shared_gate, shared_up)
    shared = grouped_product(shared_hidden, shared_down)
    expert_out = root_norm(routed + shared, exit_gain).astype(jnp.bfloat16)
    return (mixer_out, expert_out)
```

```python
import jax
import jax.numpy as jnp
from jax import lax
from jax.experimental import pallas as pl
from jax.experimental.pallas import tpu as pltpu
from jax.sharding import PartitionSpec as P

EPS = 1e-06


def in_one_piece(arrays, axis, dim, along):
    widths = [a.shape[along] for a in arrays]
    both = jnp.concatenate(arrays, axis=along)
    filled = lax.all_gather(both, axis, axis=dim, tiled=True)
    return tuple(jnp.split(filled, [sum(widths[:k]) for k in range(1, len(widths))], axis=along))


def in_blocks(array, dim, peers):
    before, after = (array.shape[:dim], array.shape[dim + 1 :])
    return jnp.moveaxis(array.reshape(*before, peers, -1, *after), dim, 0)


def sum_at_owner(array, axis, dim):
    peers = lax.axis_size(axis)
    tiles = lax.all_to_all(in_blocks(array, dim, peers), axis, 0, 0, tiled=True)
    return jnp.sum(tiles.astype(jnp.float32), axis=0)


def root_norm(values, gain_row):
    return values * lax.rsqrt(jnp.mean(values * values, axis=-1, keepdims=True) + EPS) * gain_row


def rounded_term(partial_value):
    return lax.optimization_barrier(partial_value.astype(jnp.bfloat16)).astype(jnp.float32)


LOG2E = 1.4426950408889634


def stick_block(query, block_keys, block_values, bias, carry, tri, mask):
    scores = lax.dot_general(query, block_keys, (((1,), (1,)), ((), ())), preferred_element_type=jnp.float32)
    level = (scores + bias) * LOG2E
    fail = jnp.maximum(level, 0.0) + jnp.log2(1.0 + jnp.exp2(-jnp.abs(level)))
    if mask is not None:
        counted = jnp.where(mask, fail, 0.0)
    else:
        counted = fail
    sums = jnp.dot(counted.astype(jnp.bfloat16), tri, preferred_element_type=jnp.float32)
    keys = block_keys.shape[0]
    both = jnp.concatenate([carry] * (keys // 128), axis=1)
    weights = jnp.exp2((level - fail) - (sums[:, :keys] + both))
    if mask is not None:
        weights = jnp.where(mask, weights, 0.0)
    out = jnp.dot(weights.astype(jnp.bfloat16), block_values, preferred_element_type=jnp.float32)
    return out, carry + sums[:, keys:]


KEY_TILE = 256


def attend_kernel(heads, shard_ref, query_ref, keys_ref, values_ref, bias_ref, tri_ref, out_ref):
    rows = query_ref.shape[0]
    size = query_ref.shape[1] // heads
    pair = 128 // size
    first_row = shard_ref[0] * rows
    own_tile = first_row // KEY_TILE
    tri = tri_ref[...]
    lane = lax.broadcasted_iota(jnp.int32, (rows, 128), 1)
    queries = []
    for head in range(heads):
        group = query_ref[:, (head // pair) * 128 : (head // pair + 1) * 128] * size**-0.5
        queries.append(jnp.where(lane // size == head % pair, group, 0).astype(jnp.bfloat16))

    def one_tile(tile, state, masked):
        start = pl.multiple_of(tile * KEY_TILE, KEY_TILE)
        if masked:
            key_pos = start + lax.broadcasted_iota(jnp.int32, (rows, KEY_TILE), 1)
            query_pos = first_row + lax.broadcasted_iota(jnp.int32, (rows, KEY_TILE), 0)
            mask = key_pos < query_pos
        else:
            mask = None
        outs, carries = [], []
        for head in range(heads):
            columns = slice((head // pair) * 128, (head // pair + 1) * 128)
            out, carry = stick_block(
                queries[head],
                keys_ref[pl.ds(start, KEY_TILE), columns],
                values_ref[pl.ds(start, KEY_TILE), columns],
                bias_ref[head : head + 1, pl.ds(start, KEY_TILE)],
                state[1][head],
                tri,
                mask,
            )
            outs.append(state[0][head] + out)
            carries.append(carry)
        return (tuple(outs), tuple(carries))

    zero = tuple(jnp.zeros((rows, 128), jnp.float32) for _ in range(heads))
    state = one_tile(own_tile, (zero, zero), True)
    outs, _ = lax.fori_loop(0, own_tile, lambda turn, state: one_tile(own_tile - 1 - turn, state, False), state)
    for group in range(heads // pair):
        merged = outs[group * pair]
        for other in range(1, pair):
            merged = jnp.where(lane // size == other, outs[group * pair + other], merged)
        out_ref[:, group * 128 : (group + 1) * 128] = merged.astype(jnp.bfloat16)


def attend(query_rows, all_keys, all_values, all_bias, shard):
    rows, width = query_rows.shape
    heads = all_bias.shape[1]
    row = jnp.arange(KEY_TILE)
    later = (row[:, None] > row[None, :]).astype(jnp.bfloat16)
    tri = jnp.concatenate([later, jnp.ones((KEY_TILE, 128), jnp.bfloat16)], axis=1)
    bias_rows = jnp.transpose(all_bias.astype(jnp.float32))
    vmem = pl.BlockSpec(memory_space=pltpu.VMEM)
    return pl.pallas_call(
        lambda *refs: attend_kernel(heads, *refs),
        out_shape=jax.ShapeDtypeStruct((rows, width), jnp.bfloat16),
        in_specs=[pl.BlockSpec(memory_space=pltpu.SMEM)] + [vmem] * 5,
        out_specs=vmem,
        compiler_params=pltpu.CompilerParams(vmem_limit_bytes=48 << 20),
        cost_estimate=pl.CostEstimate(flops=40_000_000_000, bytes_accessed=9_000_000, transcendentals=12_000_000),
        name="attend",
    )(jnp.full((1,), shard, jnp.int32), query_rows, all_keys, all_values, bias_rows, tri)


def shared_term_of(own_all, shared_gate, shared_up, shared_down):
    gate_part = jnp.dot(own_all, shared_gate, preferred_element_type=jnp.float32)
    up_part = jnp.dot(own_all, shared_up, preferred_element_type=jnp.float32)
    hidden = (jax.nn.silu(gate_part) * up_part).astype(jnp.bfloat16)
    return rounded_term(jnp.dot(hidden, shared_down, preferred_element_type=jnp.float32))


def on_device(
    query_rows,
    key_rows,
    value_rows,
    key_bias,
    mixer_weight,
    mixer_gain,
    routed_input,
    entry_gain,
    expert_index,
    route_weights,
    expert_gate,
    expert_up,
    expert_down,
    shared_gate,
    shared_up,
    shared_down,
    exit_gain,
):
    ep_size = lax.axis_size("ep")
    tp_size = lax.axis_size("tp")
    all_keys, all_values, all_bias = in_one_piece((key_rows, value_rows, key_bias), "ep", 0, 1)
    attended = attend(query_rows, all_keys, all_values, all_bias, lax.axis_index("ep"))
    mixer_term = rounded_term(jnp.dot(attended, mixer_weight, preferred_element_type=jnp.float32))
    row_count = routed_input.shape[0]
    top_count = expert_index.shape[1]
    local_experts = expert_gate.shape[0]
    model_width = routed_input.shape[1]
    expert_count = local_experts * ep_size
    capacity = 3 * row_count * top_count // (2 * expert_count)
    slot_total = expert_count * capacity
    normed = root_norm(routed_input.astype(jnp.float32), entry_gain).astype(jnp.bfloat16)
    flat_expert = expert_index.reshape(-1)
    onehot = (flat_expert[:, None] == jnp.arange(expert_count, dtype=jnp.int32)[None, :]).astype(
        jnp.int32
    )
    slot_rank = jnp.sum((jnp.cumsum(onehot, axis=0) - onehot) * onehot, axis=1)
    slot_index = (flat_expert * capacity + slot_rank).reshape(row_count, top_count)
    matches = slot_index[None, :, :] == jnp.arange(slot_total, dtype=jnp.int32)[:, None, None]
    selector = jnp.any(matches, axis=2).astype(jnp.bfloat16)
    outgoing = jnp.dot(selector, normed, preferred_element_type=jnp.float32).astype(jnp.bfloat16)
    outgoing = outgoing.reshape(expert_count, capacity, model_width)
    arrived = lax.all_to_all(outgoing, "ep", split_axis=0, concat_axis=0, tiled=True)
    routed_all, own_all = (
        lax.all_gather(arrived.reshape(slot_total, model_width), "tp", axis=0, tiled=True),
        lax.all_gather(normed, "tp", axis=0, tiled=True),
    )
    routed_split = routed_all.reshape(tp_size, ep_size, local_experts, capacity, model_width)
    gate_part = jnp.einsum(
        "tsecd,edf->tsecf", routed_split, expert_gate, preferred_element_type=jnp.float32
    )
    up_part = jnp.einsum(
        "tsecd,edf->tsecf", routed_split, expert_up, preferred_element_type=jnp.float32
    )
    hidden = (jax.nn.silu(gate_part) * up_part).astype(jnp.bfloat16)
    routed_term = jnp.einsum(
        "tsecf,efd->tsecd", hidden, expert_down, preferred_element_type=jnp.float32
    )
    routed_term = rounded_term(routed_term.reshape(tp_size * slot_total, model_width))
    shared_term = shared_term_of(own_all, shared_gate, shared_up, shared_down)
    mixer_sum, routed_sum, shared_sum = (
        sum_at_owner(mixer_term.astype(jnp.bfloat16), "tp", 0),
        sum_at_owner(routed_term.astype(jnp.bfloat16), "tp", 0),
        sum_at_owner(shared_term.astype(jnp.bfloat16), "tp", 0),
    )
    returned_rows = routed_sum.astype(jnp.bfloat16).reshape(expert_count, capacity, model_width)
    back_rows = lax.all_to_all(
        returned_rows, "ep", split_axis=0, concat_axis=0, tiled=True
    ).reshape(slot_total, model_width)
    gathered = back_rows[slot_index].astype(jnp.float32)
    routed = jnp.sum(route_weights[:, :, None] * gathered, axis=1)
    combined = routed + shared_sum
    expert_out = root_norm(combined, exit_gain).astype(jnp.bfloat16)
    mixer_out = root_norm(mixer_sum, mixer_gain).astype(jnp.bfloat16)
    return (mixer_out, expert_out)


def solution(mesh):
    in_specs = (
        P("ep", "tp"),
        P("ep", "tp"),
        P("ep", "tp"),
        P("ep", "tp"),
        P("tp", None),
        P(),
        P(("ep", "tp"), None),
        P(),
        P(("ep", "tp"), None),
        P(("ep", "tp"), None),
        P("ep", None, "tp"),
        P("ep", None, "tp"),
        P("ep", "tp", None),
        P(None, "tp"),
        P(None, "tp"),
        P("tp", None),
        P(),
    )
    out_specs = (P(("ep", "tp"), None), P(("ep", "tp"), None))
    return jax.shard_map(
        on_device, mesh=mesh, in_specs=in_specs, out_specs=out_specs, check_vma=False
    )
```

```python
import functools

import jax
import jax.numpy as jnp
from jax import lax
from jax.experimental import pallas as pl
from jax.experimental.pallas import tpu as pltpu
from jax.sharding import PartitionSpec as P

EPS = 1e-06


def in_one_piece(arrays, axis, dim, along):
    widths = [a.shape[along] for a in arrays]
    both = jnp.concatenate(arrays, axis=along)
    filled = lax.all_gather(both, axis, axis=dim, tiled=True)
    return tuple(jnp.split(filled, [sum(widths[:k]) for k in range(1, len(widths))], axis=along))


def in_blocks(array, dim, peers):
    before, after = (array.shape[:dim], array.shape[dim + 1 :])
    return jnp.moveaxis(array.reshape(*before, peers, -1, *after), dim, 0)


def sum_at_owner(array, axis, dim):
    peers = lax.axis_size(axis)
    tiles = lax.all_to_all(in_blocks(array, dim, peers), axis, 0, 0, tiled=True)
    return jnp.sum(tiles.astype(jnp.float32), axis=0)


def root_norm(values, gain_row):
    return values * lax.rsqrt(jnp.mean(values * values, axis=-1, keepdims=True) + EPS) * gain_row


def rounded_term(partial_value):
    return lax.optimization_barrier(partial_value.astype(jnp.bfloat16)).astype(jnp.float32)


LOG2E = 1.4426950408889634


def stick_block(query, block_keys, block_values, bias, carry, tri, mask):
    scores = lax.dot_general(query, block_keys, (((1,), (1,)), ((), ())), preferred_element_type=jnp.float32)
    level = (scores + bias) * LOG2E
    fail = jnp.maximum(level, 0.0) + jnp.log2(1.0 + jnp.exp2(-jnp.abs(level)))
    if mask is not None:
        counted = jnp.where(mask, fail, 0.0)
    else:
        counted = fail
    sums = jnp.dot(counted.astype(jnp.bfloat16), tri, preferred_element_type=jnp.float32)
    keys = block_keys.shape[0]
    both = jnp.concatenate([carry] * (keys // 128), axis=1)
    weights = jnp.exp2((level - fail) - (sums[:, :keys] + both))
    if mask is not None:
        weights = jnp.where(mask, weights, 0.0)
    out = jnp.dot(weights.astype(jnp.bfloat16), block_values, preferred_element_type=jnp.float32)
    return out, carry + sums[:, keys:]


KEY_TILE = 256


def attend_kernel(heads, shard_ref, query_ref, keys_ref, values_ref, bias_ref, tri_ref, out_ref):
    rows = query_ref.shape[0]
    size = query_ref.shape[1] // heads
    pair = 128 // size
    first_row = shard_ref[0] * rows
    own_tile = first_row // KEY_TILE
    tri = tri_ref[...]
    lane = lax.broadcasted_iota(jnp.int32, (rows, 128), 1)
    queries = []
    for head in range(heads):
        group = query_ref[:, (head // pair) * 128 : (head // pair + 1) * 128] * size**-0.5
        queries.append(jnp.where(lane // size == head % pair, group, 0).astype(jnp.bfloat16))

    def one_tile(tile, state, masked):
        start = pl.multiple_of(tile * KEY_TILE, KEY_TILE)
        if masked:
            key_pos = start + lax.broadcasted_iota(jnp.int32, (rows, KEY_TILE), 1)
            query_pos = first_row + lax.broadcasted_iota(jnp.int32, (rows, KEY_TILE), 0)
            mask = key_pos < query_pos
        else:
            mask = None
        outs, carries = [], []
        for head in range(heads):
            columns = slice((head // pair) * 128, (head // pair + 1) * 128)
            out, carry = stick_block(
                queries[head],
                keys_ref[pl.ds(start, KEY_TILE), columns],
                values_ref[pl.ds(start, KEY_TILE), columns],
                bias_ref[head : head + 1, pl.ds(start, KEY_TILE)],
                state[1][head],
                tri,
                mask,
            )
            outs.append(state[0][head] + out)
            carries.append(carry)
        return (tuple(outs), tuple(carries))

    zero = tuple(jnp.zeros((rows, 128), jnp.float32) for _ in range(heads))
    state = one_tile(own_tile, (zero, zero), True)
    outs, _ = lax.fori_loop(0, own_tile, lambda turn, state: one_tile(own_tile - 1 - turn, state, False), state)
    for group in range(heads // pair):
        merged = outs[group * pair]
        for other in range(1, pair):
            merged = jnp.where(lane // size == other, outs[group * pair + other], merged)
        out_ref[:, group * 128 : (group + 1) * 128] = merged.astype(jnp.bfloat16)


def attend(query_rows, all_keys, all_values, all_bias, shard):
    rows, width = query_rows.shape
    heads = all_bias.shape[1]
    row = jnp.arange(KEY_TILE)
    later = (row[:, None] > row[None, :]).astype(jnp.bfloat16)
    tri = jnp.concatenate([later, jnp.ones((KEY_TILE, 128), jnp.bfloat16)], axis=1)
    bias_rows = jnp.transpose(all_bias.astype(jnp.float32))
    vmem = pl.BlockSpec(memory_space=pltpu.VMEM)
    return pl.pallas_call(
        lambda *refs: attend_kernel(heads, *refs),
        out_shape=jax.ShapeDtypeStruct((rows, width), jnp.bfloat16),
        in_specs=[pl.BlockSpec(memory_space=pltpu.SMEM)] + [vmem] * 5,
        out_specs=vmem,
        compiler_params=pltpu.CompilerParams(vmem_limit_bytes=48 << 20),
        cost_estimate=pl.CostEstimate(flops=40_000_000_000, bytes_accessed=9_000_000, transcendentals=12_000_000),
        name="attend",
    )(jnp.full((1,), shard, jnp.int32), query_rows, all_keys, all_values, bias_rows, tri)


PLANE = 8
CAPACITY = 2


def silu_product(gate, up):
    return (gate / (1.0 + jnp.exp(-gate)) * up).astype(jnp.bfloat16)


def expert_kernel(
    groups,
    plane,
    outgoing,
    normed,
    gate_hbm,
    up_hbm,
    down_hbm,
    shared_gate_hbm,
    shared_up_hbm,
    shared_down_hbm,
    back,
    shared_out,
    stage,
    rows,
    partial,
    first_sum,
    second_sum,
    result,
    returned,
    neighbours,
    shared_part,
    shared_first,
    shared_second,
    gate_w,
    up_w,
    down_w,
    shared_gate_w,
    shared_up_w,
    shared_down_w,
    weight_sem,
    own_sem,
    z_send,
    z_recv,
    p_send,
    p_recv,
    x_send,
    x_recv,
    q_send,
    q_recv,
    b_send,
    b_recv,
    s_send,
    s_recv,
):
    f32, bf16 = jnp.float32, jnp.bfloat16
    own_ep = lax.axis_index("ep")
    own_x = lax.axis_index("tp")
    own_z = own_ep // plane
    own_p = own_ep % plane
    half = plane // 2
    right = (own_x + 1) % 4
    left = (own_x + 3) % 4
    side = (right, left)
    experts, width = gate_w.shape[0], gate_w.shape[1]
    shared_rows = normed.shape[0]
    shared_half = shared_rows // 2

    def remote(src, dst, send_sem, recv_sem, ep, tp):
        return pltpu.make_async_remote_copy(
            src_ref=src,
            dst_ref=dst,
            send_sem=send_sem,
            recv_sem=recv_sem,
            device_id=(ep, tp),
            device_id_type=pl.DeviceIdType.MESH,
        )

    def offset(c):
        odd = c % 2
        return (odd * ((c + 1) // 2) + (1 - odd) * (groups - c // 2)) % groups

    def z_copy(c):
        there = (own_z + offset(c)) % groups
        return remote(
            outgoing.at[there], stage.at[c], z_send.at[c], z_recv.at[c], there * plane + own_p, own_x
        )

    def p_copy(c, i):
        there = (own_p + i) % plane
        return remote(
            stage.at[c, there],
            rows.at[0, c, own_p],
            p_send.at[c, i],
            p_recv.at[c, i],
            own_z * plane + there,
            own_x,
        )

    def p_own(c):
        return pltpu.make_async_copy(stage.at[c, own_p], rows.at[0, c, own_p], own_sem.at[0, c])

    def x_copy(c, way):
        return remote(
            rows.at[0, c], rows.at[1 + way, c], x_send.at[0, way, c], x_recv.at[0, way, c], own_ep, side[way]
        )

    def f_copy(c, way):
        part = pl.ds(way * half, half)
        return remote(
            rows.at[1 + way, c, part],
            rows.at[3, c, part],
            x_send.at[1, way, c],
            x_recv.at[1, way, c],
            own_ep,
            side[way],
        )

    def r_copy(c, way):
        return remote(
            partial.at[3, c, pl.ds(way * half, half)],
            first_sum.at[way, c],
            x_send.at[2, way, c],
            x_recv.at[2, way, c],
            own_ep,
            side[way],
        )

    def t_copy(c, way):
        return remote(
            partial.at[2 - way, c],
            second_sum.at[way, c],
            x_send.at[3, way, c],
            x_recv.at[3, way, c],
            own_ep,
            side[way],
        )

    def q_copy(c, i):
        there = (own_p + i) % plane
        return remote(
            result.at[c, there],
            returned.at[c, own_p],
            q_send.at[c, i],
            q_recv.at[c, i],
            own_z * plane + there,
            own_x,
        )

    def q_own(c):
        return pltpu.make_async_copy(result.at[c, own_p], returned.at[c, own_p], own_sem.at[1, c])

    def b_copy(c):
        there = (own_z + groups - offset(c)) % groups
        return remote(
            returned.at[c], back.at[own_z], b_send.at[c], b_recv.at[c], there * plane + own_p, own_x
        )

    def shared_copy(kind, way):
        part = pl.ds(way * shared_half, shared_half)
        src, dst = (
            (normed, neighbours.at[way]),
            (neighbours.at[way, part], neighbours.at[2, part]),
            (shared_part.at[3, part], shared_first.at[way]),
            (shared_part.at[2 - way], shared_second.at[way]),
        )[kind]
        return remote(src, dst, s_send.at[kind, way], s_recv.at[kind, way], own_ep, side[way])

    first_z = pltpu.make_async_copy(outgoing.at[own_z], stage.at[0], own_sem.at[2, 0])
    last_z = pltpu.make_async_copy(returned.at[0], back.at[own_z], own_sem.at[2, 1])
    loads = [
        pltpu.make_async_copy(src, dst, weight_sem.at[n])
        for n, (src, dst) in enumerate(
            (
                (shared_gate_hbm, shared_gate_w),
                (shared_up_hbm, shared_up_w),
                (shared_down_hbm, shared_down_w),
                (gate_hbm, gate_w),
                (up_hbm, up_w),
                (down_hbm, down_w),
            )
        )
    ]

    barrier = pltpu.get_barrier_semaphore()

    def greet(ep, tp):
        pl.semaphore_signal(
            barrier, inc=1, device_id=(ep, tp), device_id_type=pl.DeviceIdType.MESH
        )

    for k in range(1, groups):
        greet(((own_z + k) % groups) * plane + own_p, own_x)
    for k in range(1, plane):
        greet(own_z * plane + (own_p + k) % plane, own_x)
    greet(own_ep, right)
    greet(own_ep, left)
    first_z.start()
    for load in loads:
        load.start()
    pl.semaphore_wait(barrier, groups + plane)

    for way in range(2):
        shared_copy(0, way).start()
    for c in range(1, groups):
        z_copy(c).start()
    first_z.wait()

    def compute_shared():
        def one_block(source, target):
            block = source[...]
            gate = jnp.dot(block, shared_gate_w[...], preferred_element_type=f32)
            up = jnp.dot(block, shared_up_w[...], preferred_element_type=f32)
            hidden = silu_product(gate, up)
            target[...] = jnp.dot(hidden, shared_down_w[...], preferred_element_type=f32).astype(bf16)

        one_block(normed, shared_part.at[0])
        for j in range(3):
            one_block(neighbours.at[j], shared_part.at[j + 1])

    def compute_rows(c):
        count = 4 * plane * CAPACITY
        for e in range(experts):
            block = rows[:, c, :, e].reshape(count, width)
            gate = jnp.dot(block, gate_w[e], preferred_element_type=f32)
            up = jnp.dot(block, up_w[e], preferred_element_type=f32)
            hidden = silu_product(gate, up)
            product = jnp.dot(hidden, down_w[e], preferred_element_type=f32).astype(bf16)
            partial[:, c, :, e] = product.reshape(4, plane, CAPACITY, width)

    def flat(value):
        return value.reshape(-1, width).astype(f32)

    def add_first(c):
        for way in range(2):
            part = pl.ds(way * half, half)
            total = flat(partial[2 - way, c, part]) + flat(first_sum[way, c])
            partial[2 - way, c, part] = total.astype(bf16).reshape(half, experts, CAPACITY, width)

    def add_second(c):
        total = flat(partial[0, c]) + flat(second_sum[0, c]) + flat(second_sum[1, c])
        result[c] = total.astype(bf16).reshape(plane, experts, CAPACITY, width)

    def step(s, unused):
        @pl.when(s < groups)
        def _():
            @pl.when(s > 0)
            def _():
                z_copy(s).wait_recv()

            p_own(s).start()
            for i in range(1, plane):
                p_copy(s, i).start()

        @pl.when(s == 2)
        def _():
            for way in range(2):
                shared_copy(0, way).wait_recv()
                shared_copy(1, way).start()

        @pl.when((s >= 1) & (s < groups + 1))
        def _():
            c = s - 1
            for i in range(1, plane):
                p_copy(c, i).wait_recv()
            p_own(c).wait()
            for way in range(2):
                x_copy(c, way).start()

        @pl.when((s >= 2) & (s < groups + 2))
        def _():
            c = s - 2
            for way in range(2):
                x_copy(c, way).wait_recv()
                f_copy(c, way).start()

        @pl.when(s == 3)
        def _():
            for load in loads:
                load.wait()
            for way in range(2):
                shared_copy(1, way).wait_recv()
            compute_shared()

        @pl.when((s >= 3) & (s < groups + 3))
        def _():
            c = s - 3
            for way in range(2):
                f_copy(c, way).wait_recv()
            compute_rows(c)
            for way in range(2):
                r_copy(c, way).start()

        @pl.when(s == groups)
        def _():
            for way in range(2):
                shared_copy(2, way).start()

        @pl.when((s >= 4) & (s < groups + 4))
        def _():
            c = s - 4
            for way in range(2):
                r_copy(c, way).wait_recv()
            add_first(c)
            for way in range(2):
                t_copy(c, way).start()

        @pl.when(s == groups + 1)
        def _():
            for way in range(2):
                shared_copy(2, way).wait_recv()
                part = pl.ds(way * shared_half, shared_half)
                shared_part[2 - way, part] = (
                    shared_part[2 - way, part].astype(f32) + shared_first[way].astype(f32)
                ).astype(bf16)
            for way in range(2):
                shared_copy(3, way).start()

        @pl.when((s >= 5) & (s < groups + 5))
        def _():
            c = s - 5
            for way in range(2):
                t_copy(c, way).wait_recv()
            add_second(c)
            q_own(c).start()
            for i in range(1, plane):
                q_copy(c, i).start()

        @pl.when((s >= 6) & (s < groups + 6))
        def _():
            c = s - 6
            for i in range(1, plane):
                q_copy(c, i).wait_recv()
            q_own(c).wait()

            @pl.when(c > 0)
            def _():
                b_copy(c).start()

            @pl.when(c == 0)
            def _():
                last_z.start()

        return unused

    lax.fori_loop(0, groups + 6, step, 0)

    for way in range(2):
        shared_copy(3, way).wait_recv()
    shared_out[...] = (
        shared_part[0].astype(f32) + shared_second[0].astype(f32) + shared_second[1].astype(f32)
    )

    def drain(c, unused):
        for i in range(1, plane):
            p_copy(c, i).wait_send()
            q_copy(c, i).wait_send()
        for way in range(2):
            for copy in (x_copy, f_copy, r_copy, t_copy):
                copy(c, way).wait_send()

        @pl.when(c > 0)
        def _():
            z_copy(c).wait_send()
            b_copy(c).wait_send()
            b_copy(c).wait_recv()

        return unused

    lax.fori_loop(0, groups, drain, 0)
    for kind in range(4):
        for way in range(2):
            shared_copy(kind, way).wait_send()
    last_z.wait()


def exchange_and_expand(outgoing, normed, gate, up, down, shared_gate, shared_up, shared_down):
    groups, plane, experts, capacity, width = outgoing.shape
    count = normed.shape[0]
    half = plane // 2
    bf16 = jnp.bfloat16
    block = (plane, experts, capacity, width)
    vmem = pl.BlockSpec(memory_space=pltpu.VMEM)
    hbm = pl.BlockSpec(memory_space=pl.ANY)
    weights = (gate, up, down, shared_gate, shared_up, shared_down)
    dma = pltpu.SemaphoreType.DMA
    return pl.pallas_call(
        functools.partial(expert_kernel, groups, plane),
        out_shape=(
            jax.ShapeDtypeStruct(outgoing.shape, bf16),
            jax.ShapeDtypeStruct(normed.shape, jnp.float32),
        ),
        in_specs=[vmem, vmem] + [hbm] * 6,
        out_specs=(vmem, vmem),
        scratch_shapes=[
            pltpu.VMEM((groups,) + block, bf16),
            pltpu.VMEM((4, groups) + block, bf16),
            pltpu.VMEM((4, groups) + block, bf16),
            pltpu.VMEM((2, groups, half) + block[1:], bf16),
            pltpu.VMEM((2, groups) + block, bf16),
            pltpu.VMEM((groups,) + block, bf16),
            pltpu.VMEM((groups,) + block, bf16),
            pltpu.VMEM((3, count, width), bf16),
            pltpu.VMEM((4, count, width), bf16),
            pltpu.VMEM((2, count // 2, width), bf16),
            pltpu.VMEM((2, count, width), bf16),
        ]
        + [pltpu.VMEM(w.shape, bf16) for w in weights]
        + [
            dma((6,)),
            dma((3, groups)),
            dma((groups,)),
            dma((groups,)),
            dma((groups, plane)),
            dma((groups, plane)),
            dma((4, 2, groups)),
            dma((4, 2, groups)),
            dma((groups, plane)),
            dma((groups, plane)),
            dma((groups,)),
            dma((groups,)),
            dma((4, 2)),
            dma((4, 2)),
        ],
        compiler_params=pltpu.CompilerParams(
            collective_id=1, has_side_effects=True, vmem_limit_bytes=60 << 20
        ),
        name="experts",
    )(outgoing, normed, *weights)


def expert_layer(
    routed_input,
    entry_gain,
    expert_index,
    route_weights,
    expert_gate,
    expert_up,
    expert_down,
    shared_gate,
    shared_up,
    shared_down,
    exit_gain,
):
    ep_size = lax.axis_size("ep")
    row_count, top_count = expert_index.shape
    local_experts = expert_gate.shape[0]
    model_width = routed_input.shape[1]
    expert_count = local_experts * ep_size
    slot_total = expert_count * CAPACITY
    normed = root_norm(routed_input.astype(jnp.float32), entry_gain).astype(jnp.bfloat16)
    flat_expert = expert_index.reshape(-1)
    onehot = (flat_expert[:, None] == jnp.arange(expert_count, dtype=jnp.int32)[None, :]).astype(
        jnp.int32
    )
    slot_rank = jnp.sum((jnp.cumsum(onehot, axis=0) - onehot) * onehot, axis=1)
    slot_index = (flat_expert * CAPACITY + slot_rank).reshape(row_count, top_count)
    matches = slot_index[None, :, :] == jnp.arange(slot_total, dtype=jnp.int32)[:, None, None]
    selector = jnp.any(matches, axis=2).astype(jnp.bfloat16)
    outgoing = jnp.dot(selector, normed, preferred_element_type=jnp.float32).astype(jnp.bfloat16)
    outgoing = outgoing.reshape(ep_size // PLANE, PLANE, local_experts, CAPACITY, model_width)
    back, shared_sum = exchange_and_expand(
        outgoing, normed, expert_gate, expert_up, expert_down, shared_gate, shared_up, shared_down
    )
    back_rows = back.reshape(slot_total, model_width)
    gathered = back_rows[slot_index].astype(jnp.float32)
    routed = jnp.sum(route_weights[:, :, None] * gathered, axis=1)
    return root_norm(routed + shared_sum, exit_gain).astype(jnp.bfloat16)


def on_device(
    query_rows,
    key_rows,
    value_rows,
    key_bias,
    mixer_weight,
    mixer_gain,
    routed_input,
    entry_gain,
    expert_index,
    route_weights,
    expert_gate,
    expert_up,
    expert_down,
    shared_gate,
    shared_up,
    shared_down,
    exit_gain,
):
    all_keys, all_values, all_bias = in_one_piece((key_rows, value_rows, key_bias), "ep", 0, 1)
    attended = attend(query_rows, all_keys, all_values, all_bias, lax.axis_index("ep"))
    mixer_term = rounded_term(jnp.dot(attended, mixer_weight, preferred_element_type=jnp.float32))
    mixer_sum = sum_at_owner(mixer_term.astype(jnp.bfloat16), "tp", 0)
    expert_out = expert_layer(
        routed_input,
        entry_gain,
        expert_index,
        route_weights,
        expert_gate,
        expert_up,
        expert_down,
        shared_gate,
        shared_up,
        shared_down,
        exit_gain,
    )
    mixer_out = root_norm(mixer_sum, mixer_gain).astype(jnp.bfloat16)
    return (mixer_out, expert_out)


def solution(mesh):
    in_specs = (
        P("ep", "tp"),
        P("ep", "tp"),
        P("ep", "tp"),
        P("ep", "tp"),
        P("tp", None),
        P(),
        P(("ep", "tp"), None),
        P(),
        P(("ep", "tp"), None),
        P(("ep", "tp"), None),
        P("ep", None, "tp"),
        P("ep", None, "tp"),
        P("ep", "tp", None),
        P(None, "tp"),
        P(None, "tp"),
        P("tp", None),
        P(),
    )
    out_specs = (P(("ep", "tp"), None), P(("ep", "tp"), None))
    return jax.shard_map(
        on_device, mesh=mesh, in_specs=in_specs, out_specs=out_specs, check_vma=False
    )
```

```python
import functools

import jax
import jax.numpy as jnp
from jax import lax
from jax.experimental import pallas as pl
from jax.experimental.pallas import tpu as pltpu
from jax.sharding import PartitionSpec as P

EPS = 1e-06
LOG2E = 1.4426950408889634
PLANE = 8
CAPACITY = 2


def root_norm(values, gain_row):
    return values * lax.rsqrt(jnp.mean(values * values, axis=-1, keepdims=True) + EPS) * gain_row


def stick_block(query, block_keys, block_values, bias, carry, tri, mask):
    scores = lax.dot_general(query, block_keys, (((1,), (1,)), ((), ())), preferred_element_type=jnp.float32)
    level = (scores + bias) * LOG2E
    fail = jnp.maximum(level, 0.0) + jnp.log2(1.0 + jnp.exp2(-jnp.abs(level)))
    if mask is not None:
        counted = jnp.where(mask, fail, 0.0)
    else:
        counted = fail
    sums = jnp.dot(counted.astype(jnp.bfloat16), tri, preferred_element_type=jnp.float32)
    keys = block_keys.shape[0]
    both = jnp.concatenate([carry] * (keys // 128), axis=1)
    weights = jnp.exp2((level - fail) - (sums[:, :keys] + both))
    if mask is not None:
        weights = jnp.where(mask, weights, 0.0)
    out = jnp.dot(weights.astype(jnp.bfloat16), block_values, preferred_element_type=jnp.float32)
    return out, carry + sums[:, keys:]


KEY_TILE = 256


def silu_product(gate, up):
    return (gate / (1.0 + jnp.exp(-gate)) * up).astype(jnp.bfloat16)


def program_kernel(
    groups,
    plane,
    query_ref,
    key_ref,
    value_ref,
    bias_ref,
    tri_ref,
    mixer_hbm,
    mixer_gain_ref,
    input_ref,
    entry_gain_ref,
    index_ref,
    weight_ref,
    exit_gain_ref,
    gate_hbm,
    up_hbm,
    down_hbm,
    shared_gate_hbm,
    shared_up_hbm,
    shared_down_hbm,
    mixer_out,
    expert_out,
    normed,
    outgoing,
    back,
    stage,
    rows,
    partial,
    first_sum,
    second_sum,
    result,
    returned,
    neighbours,
    shared_part,
    shared_first,
    shared_second,
    kv_own,
    query_own,
    kv_all,
    queries,
    running,
    carried,
    far_part,
    attended_back,
    attended,
    mixer_part,
    mixer_first,
    mixer_second,
    mixer_w,
    gate_w,
    up_w,
    down_w,
    shared_gate_w,
    shared_up_w,
    shared_down_w,
    mixing_high,
    mixing_low,
    shared_total,
    weight_sem,
    own_sem,
    z_send,
    z_recv,
    p_send,
    p_recv,
    x_send,
    x_recv,
    q_send,
    q_recv,
    b_send,
    b_recv,
    s_send,
    s_recv,
    a_send,
    a_recv,
):
    f32, bf16 = jnp.float32, jnp.bfloat16
    own_ep = lax.axis_index("ep")
    own_x = lax.axis_index("tp")
    own_z = own_ep // plane
    own_p = own_ep % plane
    own_y = own_p // 2
    own_core = own_p % 2
    lines = plane // 2
    half = plane // 2
    right = (own_x + 1) % 4
    left = (own_x + 3) % 4
    opposite = (own_x + 2) % 4
    side = (right, left)
    experts, width = gate_w.shape[0], gate_w.shape[1]
    shared_rows = normed.shape[0]
    shared_half = shared_rows // 2
    tokens = key_ref.shape[0]
    head_size = query_ref.shape[1] // lines
    mixer_rows = tokens // 4
    mixer_half = mixer_rows // 2
    slots = groups * plane * experts * CAPACITY

    def remote(src, dst, send_sem, recv_sem, ep, tp):
        return pltpu.make_async_remote_copy(
            src_ref=src,
            dst_ref=dst,
            send_sem=send_sem,
            recv_sem=recv_sem,
            device_id=(ep, tp),
            device_id_type=pl.DeviceIdType.MESH,
        )

    def offset(c):
        odd = c % 2
        return (odd * ((c + 1) // 2) + (1 - odd) * (groups - c // 2)) % groups

    def z_copy(c):
        there = (own_z + offset(c)) % groups
        return remote(
            outgoing.at[there], stage.at[c], z_send.at[c], z_recv.at[c], there * plane + own_p, own_x
        )

    def p_copy(c, i):
        there = (own_p + i) % plane
        return remote(
            stage.at[c, there],
            rows.at[0, c, own_p],
            p_send.at[c, i],
            p_recv.at[c, i],
            own_z * plane + there,
            own_x,
        )

    def p_own(c):
        return pltpu.make_async_copy(stage.at[c, own_p], rows.at[0, c, own_p], own_sem.at[0, c])

    def x_copy(c, way):
        return remote(
            rows.at[0, c], rows.at[1 + way, c], x_send.at[0, way, c], x_recv.at[0, way, c], own_ep, side[way]
        )

    def f_copy(c, way):
        part = pl.ds(way * half, half)
        return remote(
            rows.at[1 + way, c, part],
            rows.at[3, c, part],
            x_send.at[1, way, c],
            x_recv.at[1, way, c],
            own_ep,
            side[way],
        )

    def r_copy(c, way):
        return remote(
            partial.at[3, c, pl.ds(way * half, half)],
            first_sum.at[way, c],
            x_send.at[2, way, c],
            x_recv.at[2, way, c],
            own_ep,
            side[way],
        )

    def t_copy(c, way):
        return remote(
            partial.at[2 - way, c],
            second_sum.at[way, c],
            x_send.at[3, way, c],
            x_recv.at[3, way, c],
            own_ep,
            side[way],
        )

    def q_copy(c, i):
        there = (own_p + i) % plane
        return remote(
            result.at[c, there],
            returned.at[c, own_p],
            q_send.at[c, i],
            q_recv.at[c, i],
            own_z * plane + there,
            own_x,
        )

    def q_own(c):
        return pltpu.make_async_copy(result.at[c, own_p], returned.at[c, own_p], own_sem.at[1, c])

    def b_copy(c):
        there = (own_z + groups - offset(c)) % groups
        return remote(
            returned.at[c], back.at[own_z], b_send.at[c], b_recv.at[c], there * plane + own_p, own_x
        )

    def shared_copy(kind, way):
        part = pl.ds(way * shared_half, shared_half)
        src, dst = (
            (normed, neighbours.at[way]),
            (neighbours.at[way, part], neighbours.at[2, part]),
            (shared_part.at[3, part], shared_first.at[way]),
            (shared_part.at[2 - way], shared_second.at[way]),
        )[kind]
        return remote(src, dst, s_send.at[kind, way], s_recv.at[kind, way], own_ep, side[way])

    mirror = (groups - 1 - own_z) * plane + own_p
    partner = own_z * plane + own_p + 1 - 2 * own_core

    def k_copy(i):
        line = (own_y + i) % lines
        return remote(
            kv_own.at[line],
            kv_all.at[own_z, own_core, own_y],
            a_send.at[0, i],
            a_recv.at[0, i],
            own_z * plane + 2 * line + own_core,
            own_x,
        )

    def ask_copy(i):
        line = (own_y + i) % lines
        return remote(
            query_own.at[line],
            queries.at[own_y],
            a_send.at[1, i],
            a_recv.at[1, i],
            own_z * plane + 2 * line + own_core,
            own_x,
        )

    def kz_copy(c):
        there = (own_z + offset(c)) % groups
        block = kv_all.at[own_z, own_core]
        return remote(block, block, a_send.at[2, c], a_recv.at[2, c], there * plane + own_p, own_x)

    def kd_copy(c):
        source = (own_z + groups - offset(c)) % groups
        block = kv_all.at[source, own_core]
        return remote(block, block, a_send.at[3, c], a_recv.at[3, c], partner, own_x)

    def answer_copy(i):
        line = (own_y + i) % lines
        return remote(
            attended_back.at[line],
            attended.at[own_y],
            a_send.at[4, i],
            a_recv.at[4, i],
            own_z * plane + 2 * line + own_core,
            own_x,
        )

    ask_far = remote(
        queries.at[pl.ds(2, 2)], queries.at[pl.ds(4, 2)], a_send.at[5, 0], a_recv.at[5, 0], mirror, own_x
    )
    answer_far = remote(
        far_part, attended_back.at[pl.ds(2, 2)], a_send.at[5, 1], a_recv.at[5, 1], mirror, own_x
    )
    k_own = pltpu.make_async_copy(
        kv_own.at[own_y], kv_all.at[own_z, own_core, own_y], own_sem.at[2, 2]
    )
    ask_own = pltpu.make_async_copy(query_own.at[own_y], queries.at[own_y], own_sem.at[2, 3])
    answer_own = pltpu.make_async_copy(
        attended_back.at[own_y], attended.at[own_y], own_sem.at[2, 4]
    )

    def mixer_copy(kind, way):
        part = pl.ds(way * mixer_half, mixer_half)
        src, dst = (
            (mixer_part.at[opposite, part], mixer_first.at[way]),
            (mixer_part.at[side[way]], mixer_second.at[way]),
        )[kind]
        return remote(src, dst, s_send.at[4 + kind, way], s_recv.at[4 + kind, way], own_ep, side[way])

    first_z = pltpu.make_async_copy(outgoing.at[own_z], stage.at[0], own_sem.at[2, 0])
    last_z = pltpu.make_async_copy(returned.at[0], back.at[own_z], own_sem.at[2, 1])
    loads = [
        pltpu.make_async_copy(src, dst, weight_sem.at[n])
        for n, (src, dst) in enumerate(
            (
                (shared_gate_hbm, shared_gate_w),
                (shared_up_hbm, shared_up_w),
                (shared_down_hbm, shared_down_w),
                (gate_hbm, gate_w),
                (up_hbm, up_w),
                (down_hbm, down_w),
                (mixer_hbm, mixer_w),
            )
        )
    ]

    barrier = pltpu.get_barrier_semaphore()

    def greet(ep, tp):
        pl.semaphore_signal(
            barrier, inc=1, device_id=(ep, tp), device_id_type=pl.DeviceIdType.MESH
        )

    for k in range(1, groups):
        greet(((own_z + k) % groups) * plane + own_p, own_x)
    for k in range(1, plane):
        greet(own_z * plane + (own_p + k) % plane, own_x)
    greet(own_ep, right)
    greet(own_ep, left)
    for load in loads:
        load.start()

    normed[...] = root_norm(input_ref[...].astype(f32), entry_gain_ref[...]).astype(bf16)

    lane = lax.broadcasted_iota(jnp.int32, (tokens, 128), 1)
    low = lane < head_size
    eye = (lax.broadcasted_iota(jnp.int32, (tokens, tokens), 0) == lax.broadcasted_iota(
        jnp.int32, (tokens, tokens), 1
    )).astype(bf16)
    bias_rows = lax.dot_general(
        bias_ref[...], eye, (((0,), (0,)), ((), ())), preferred_element_type=f32
    )
    for head in range(lines):
        column = (head // 2) * 128

        def placed(ref, upper):
            group = ref[:, column : column + 128].astype(f32)
            return group if head % 2 == upper else pltpu.roll(group, head_size, 1)

        kv_own[head, :tokens] = jnp.where(low, placed(key_ref, 0), placed(value_ref, 1)).astype(bf16)
        kv_own[head, tokens:] = jnp.broadcast_to(bias_rows[head : head + 1], (16, 128)).astype(bf16)
        query_own[head] = jnp.where(low, placed(query_ref, 0) * head_size**-0.5, 0.0).astype(bf16)

    expert_lane = lax.broadcasted_iota(jnp.int32, (shared_rows, slots // CAPACITY), 1)
    slot_lane = lax.broadcasted_iota(jnp.int32, (shared_rows, slots), 1)
    named = [(expert_lane == index_ref[:, k : k + 1]).astype(f32) for k in range(2)]
    earlier = (
        lax.broadcasted_iota(jnp.int32, (shared_rows, shared_rows), 1)
        < lax.broadcasted_iota(jnp.int32, (shared_rows, shared_rows), 0)
    ).astype(bf16)
    before = jnp.dot(earlier, (named[0] + named[1]).astype(bf16), preferred_element_type=f32)

    def placed_in(k):
        rank = jnp.sum(named[k] * before, axis=1, keepdims=True).astype(jnp.int32)
        return slot_lane == index_ref[:, k : k + 1] * CAPACITY + rank

    chosen = [placed_in(k) for k in range(2)]
    selector = (chosen[0] | chosen[1]).astype(f32).astype(bf16)
    mixing = jnp.where(chosen[0], weight_ref[:, 0:1], 0.0) + jnp.where(
        chosen[1], weight_ref[:, 1:2], 0.0
    )
    mixing_high[...] = mixing.astype(bf16)
    mixing_low[...] = (mixing - mixing.astype(bf16).astype(f32)).astype(bf16)
    outgoing[...] = (
        lax.dot_general(
            selector, normed[...], (((0,), (0,)), ((), ())), preferred_element_type=f32
        )
        .astype(bf16)
        .reshape(outgoing.shape)
    )
    running[...] = jnp.zeros_like(running)
    carried[...] = jnp.zeros_like(carried)
    first_z.start()
    k_own.start()
    ask_own.start()
    pl.semaphore_wait(barrier, groups + plane)

    for way in range(2):
        shared_copy(0, way).start()
    for c in range(1, min(groups, 5)):
        z_copy(c).start()
    for i in range(1, lines):
        k_copy(i).start()
        ask_copy(i).start()
    first_z.wait()

    def compute_shared():
        def one_block(source, target):
            block = source[...]
            gate = jnp.dot(block, shared_gate_w[...], preferred_element_type=f32)
            up = jnp.dot(block, shared_up_w[...], preferred_element_type=f32)
            hidden = silu_product(gate, up)
            target[...] = jnp.dot(hidden, shared_down_w[...], preferred_element_type=f32).astype(bf16)

        one_block(normed, shared_part.at[0])
        for j in range(3):
            one_block(neighbours.at[j], shared_part.at[j + 1])

    def compute_rows(c):
        count = 4 * plane * CAPACITY
        for e in range(experts):
            block = rows[:, c, :, e].reshape(count, width)
            gate = jnp.dot(block, gate_w[e], preferred_element_type=f32)
            up = jnp.dot(block, up_w[e], preferred_element_type=f32)
            hidden = silu_product(gate, up)
            product = jnp.dot(hidden, down_w[e], preferred_element_type=f32).astype(bf16)
            partial[:, c, :, e] = product.reshape(4, plane, CAPACITY, width)

    def flat(value):
        return value.reshape(-1, width).astype(f32)

    def add_first(c):
        for way in range(2):
            part = pl.ds(way * half, half)
            total = flat(partial[2 - way, c, part]) + flat(first_sum[way, c])
            partial[2 - way, c, part] = total.astype(bf16).reshape(half, experts, CAPACITY, width)

    def add_second(c):
        total = flat(partial[0, c]) + flat(second_sum[0, c]) + flat(second_sum[1, c])
        result[c] = total.astype(bf16).reshape(plane, experts, CAPACITY, width)

    first_turns = lines * own_z + 2
    turns = lines * (groups - 1) + 6
    share = (turns + 3) // 4

    def attend_turn(turn, unused):
        second = jnp.where(turn >= first_turns, 1, 0)
        query_z = own_z + second * (groups - 1 - 2 * own_z)
        tile = (1 - second) * (first_turns - 1 - turn) + second * (
            lines * query_z + 3 - (turn - first_turns)
        )
        tile_z = tile // lines
        tile_y = tile % lines
        limit = ((query_z * lines + 2 * second) * 2 + own_core) * tokens - tile * 2 * tokens
        row = lax.broadcasted_iota(jnp.int32, (2 * tokens, 2 * tokens), 0)
        column = lax.broadcasted_iota(jnp.int32, (2 * tokens, 2 * tokens), 1)
        mask = column - (row + (row // tokens) * tokens) < limit
        query = queries[pl.ds(4 * second, 2)].reshape(2 * tokens, 128)
        blocks = [kv_all[tile_z, core, tile_y] for core in range(2)]
        block = jnp.concatenate([b[:tokens] for b in blocks], axis=0)
        bias = jnp.concatenate([b[tokens:][:1] for b in blocks], axis=1).astype(f32)
        out, carry = stick_block(query, block, block, bias, carried[second], tri_ref[...], mask)
        running[second] = running[second] + out
        carried[second] = carry
        return unused

    def finish_attention():
        low2 = lax.broadcasted_iota(jnp.int32, (2 * tokens, 128), 1) < head_size
        even = own_y % 2 == 0
        for second, target in ((0, attended_back.at[pl.ds(0, 2)]), (1, far_part)):
            value = running[second]
            value = jnp.where(even, pltpu.roll(value, head_size, 1), value)
            target[...] = value.astype(bf16).reshape(2, tokens, 128)

    def mix():
        low1 = lax.broadcasted_iota(jnp.int32, (tokens, 128), 1) < head_size
        groups_of_two = [
            jnp.where(low1, attended[2 * n].astype(f32), attended[2 * n + 1].astype(f32)).astype(bf16)
            for n in range(lines // 2)
        ]
        gathered = jnp.concatenate(groups_of_two, axis=1)
        product = jnp.dot(gathered, mixer_w[...], preferred_element_type=f32).astype(bf16)
        mixer_part[...] = product.reshape(4, mixer_rows, width)

    def step(s, unused):
        @pl.when(s < groups)
        def _():
            @pl.when(s > 0)
            def _():
                z_copy(s).wait_recv()

            p_own(s).start()
            for i in range(1, plane):
                p_copy(s, i).start()

        @pl.when(s == 1)
        def _():
            for i in range(1, lines):
                k_copy(i).wait_recv()
            k_own.wait()
            for c in range(1, min(groups, 3)):
                kz_copy(c).start()
            for c in range(5, groups):
                z_copy(c).start()
            for c in range(3, groups):
                kz_copy(c).start()
            kd_copy(0).start()
            for i in range(1, lines):
                ask_copy(i).wait_recv()
            ask_own.wait()
            ask_far.start()

        @pl.when(s == 2)
        def _():
            for way in range(2):
                shared_copy(0, way).wait_recv()
                shared_copy(1, way).start()

        @pl.when((s >= 1) & (s < groups + 1))
        def _():
            c = s - 1
            for i in range(1, plane):
                p_copy(c, i).wait_recv()
            p_own(c).wait()
            for way in range(2):
                x_copy(c, way).start()

        @pl.when((s >= 2) & (s < groups + 2))
        def _():
            c = s - 2
            for way in range(2):
                x_copy(c, way).wait_recv()
                f_copy(c, way).start()

        @pl.when(s == 3)
        def _():
            for load in loads:
                load.wait()
            for way in range(2):
                shared_copy(1, way).wait_recv()
            compute_shared()

        @pl.when((s >= 3) & (s < groups + 3))
        def _():
            c = s - 3
            for way in range(2):
                f_copy(c, way).wait_recv()
            compute_rows(c)
            for way in range(2):
                r_copy(c, way).start()

        @pl.when(s == max(groups, 4))
        def _():
            for way in range(2):
                shared_copy(2, way).start()

        @pl.when((s >= 4) & (s < groups + 4))
        def _():
            c = s - 4
            for way in range(2):
                r_copy(c, way).wait_recv()
            add_first(c)
            for way in range(2):
                t_copy(c, way).start()

        @pl.when(s == max(groups, 4) + 1)
        def _():
            for way in range(2):
                shared_copy(2, way).wait_recv()
                part = pl.ds(way * shared_half, shared_half)
                shared_part[2 - way, part] = (
                    shared_part[2 - way, part].astype(f32) + shared_first[way].astype(f32)
                ).astype(bf16)
            for way in range(2):
                shared_copy(3, way).start()

        @pl.when((s >= 5) & (s < groups + 5))
        def _():
            c = s - 5
            for way in range(2):
                t_copy(c, way).wait_recv()
            add_second(c)
            q_own(c).start()
            for i in range(1, plane):
                q_copy(c, i).start()

        @pl.when((s >= 6) & (s < groups + 6))
        def _():
            c = s - 6
            for i in range(1, plane):
                q_copy(c, i).wait_recv()
            q_own(c).wait()

            @pl.when(c > 0)
            def _():
                b_copy(c).start()

            @pl.when(c == 0)
            def _():
                last_z.start()

        @pl.when((s >= 3) & (s < 7))
        def _():
            for n in range(2):
                c = 2 * (s - 3) + n

                @pl.when((c > 0) & (c < groups))
                def _():
                    kz_copy(c).wait_recv()
                    kd_copy(c).start()

        @pl.when(s == 7)
        def _():
            for c in range(groups):
                kd_copy(c).wait_recv()
            ask_far.wait_recv()

        @pl.when((s >= 7) & (s < 11))
        def _():
            first = (s - 7) * share
            lax.fori_loop(first, jnp.minimum(first + share, turns), attend_turn, 0)

        @pl.when(s == 10)
        def _():
            finish_attention()
            answer_far.start()

        @pl.when(s == 11)
        def _():
            answer_far.wait_recv()
            answer_own.start()
            for i in range(1, lines):
                answer_copy(i).start()

        @pl.when(s == 12)
        def _():
            for i in range(1, lines):
                answer_copy(i).wait_recv()
            answer_own.wait()
            mix()
            for way in range(2):
                mixer_copy(0, way).start()

        @pl.when(s == 13)
        def _():
            for way in range(2):
                mixer_copy(0, way).wait_recv()
                part = pl.ds(way * mixer_half, mixer_half)
                mixer_part[side[way], part] = (
                    mixer_part[side[way], part].astype(f32) + mixer_first[way].astype(f32)
                ).astype(bf16)
            for way in range(2):
                mixer_copy(1, way).start()

        return unused

    lax.fori_loop(0, max(groups + 6, 14), step, 0)

    for way in range(2):
        shared_copy(3, way).wait_recv()
    shared_sum = (
        shared_part[0].astype(f32) + shared_second[0].astype(f32) + shared_second[1].astype(f32)
    )
    shared_total[...] = shared_sum
    for way in range(2):
        mixer_copy(1, way).wait_recv()
    mixer_out[...] = root_norm(
        mixer_part[own_x].astype(f32) + mixer_second[0].astype(f32) + mixer_second[1].astype(f32),
        mixer_gain_ref[...],
    ).astype(bf16)

    def drain(c, unused):
        for i in range(1, plane):
            p_copy(c, i).wait_send()
            q_copy(c, i).wait_send()
        kd_copy(c).wait_send()
        for way in range(2):
            for copy in (x_copy, f_copy, r_copy, t_copy):
                copy(c, way).wait_send()

        @pl.when(c > 0)
        def _():
            z_copy(c).wait_send()
            b_copy(c).wait_send()
            kz_copy(c).wait_send()

        return unused

    for c in range(1, groups):
        b_copy(c).wait_recv()
    last_z.wait()
    rows_back = back[...].reshape(slots, width)
    combined = (
        jnp.dot(mixing_high[...], rows_back, preferred_element_type=f32)
        + jnp.dot(mixing_low[...], rows_back, preferred_element_type=f32)
        + shared_total[...]
    )
    expert_out[...] = root_norm(combined, exit_gain_ref[...]).astype(bf16)
    lax.fori_loop(0, groups, drain, 0)
    for kind in range(4):
        for way in range(2):
            shared_copy(kind, way).wait_send()
    for way in range(2):
        for kind in range(2):
            mixer_copy(kind, way).wait_send()
    for i in range(1, lines):
        k_copy(i).wait_send()
        ask_copy(i).wait_send()
        answer_copy(i).wait_send()
    ask_far.wait_send()
    answer_far.wait_send()


def on_device(
    query_rows,
    key_rows,
    value_rows,
    key_bias,
    mixer_weight,
    mixer_gain,
    routed_input,
    entry_gain,
    expert_index,
    route_weights,
    expert_gate,
    expert_up,
    expert_down,
    shared_gate,
    shared_up,
    shared_down,
    exit_gain,
):
    bf16, f32 = jnp.bfloat16, jnp.float32
    plane = PLANE
    groups = lax.axis_size("ep") // plane
    lines, half = plane // 2, plane // 2
    tokens = query_rows.shape[0]
    count, width = routed_input.shape
    experts = expert_gate.shape[0]
    block = (plane, experts, CAPACITY, width)
    row = jnp.arange(2 * tokens)
    later = (row[:, None] > row[None, :]).astype(bf16)
    tri = jnp.concatenate([later, jnp.ones((2 * tokens, 128), bf16)], axis=1)
    vmem = pl.BlockSpec(memory_space=pltpu.VMEM)
    hbm = pl.BlockSpec(memory_space=pl.ANY)
    weights = (expert_gate, expert_up, expert_down, shared_gate, shared_up, shared_down)
    dma = pltpu.SemaphoreType.DMA
    return pl.pallas_call(
        functools.partial(program_kernel, groups, plane),
        out_shape=(
            jax.ShapeDtypeStruct((tokens // 4, width), bf16),
            jax.ShapeDtypeStruct((count, width), bf16),
        ),
        in_specs=[vmem] * 5 + [hbm] + [vmem] * 6 + [hbm] * 6,
        out_specs=(vmem, vmem),
        scratch_shapes=[
            pltpu.VMEM((count, width), bf16),
            pltpu.VMEM((groups,) + block, bf16),
            pltpu.VMEM((groups,) + block, bf16),
            pltpu.VMEM((groups,) + block, bf16),
            pltpu.VMEM((4, groups) + block, bf16),
            pltpu.VMEM((4, groups) + block, bf16),
            pltpu.VMEM((2, groups, half) + block[1:], bf16),
            pltpu.VMEM((2, groups) + block, bf16),
            pltpu.VMEM((groups,) + block, bf16),
            pltpu.VMEM((groups,) + block, bf16),
            pltpu.VMEM((3, count, width), bf16),
            pltpu.VMEM((4, count, width), bf16),
            pltpu.VMEM((2, count // 2, width), bf16),
            pltpu.VMEM((2, count, width), bf16),
            pltpu.VMEM((lines, tokens + 16, 128), bf16),
            pltpu.VMEM((lines, tokens, 128), bf16),
            pltpu.VMEM((groups, 2, lines, tokens + 16, 128), bf16),
            pltpu.VMEM((6, tokens, 128), bf16),
            pltpu.VMEM((2, 2 * tokens, 128), f32),
            pltpu.VMEM((2, 2 * tokens, 128), f32),
            pltpu.VMEM((2, tokens, 128), bf16),
            pltpu.VMEM((lines, tokens, 128), bf16),
            pltpu.VMEM((lines, tokens, 128), bf16),
            pltpu.VMEM((4, tokens // 4, width), bf16),
            pltpu.VMEM((2, tokens // 8, width), bf16),
            pltpu.VMEM((2, tokens // 4, width), bf16),
            pltpu.VMEM(mixer_weight.shape, bf16),
        ]
        + [pltpu.VMEM(w.shape, bf16) for w in weights]
        + [
            pltpu.VMEM((count, groups * plane * experts * CAPACITY), bf16),
            pltpu.VMEM((count, groups * plane * experts * CAPACITY), bf16),
            pltpu.VMEM((count, width), f32),
            dma((7,)),
            dma((3, max(groups, 5))),
            dma((groups,)),
            dma((groups,)),
            dma((groups, plane)),
            dma((groups, plane)),
            dma((4, 2, groups)),
            dma((4, 2, groups)),
            dma((groups, plane)),
            dma((groups, plane)),
            dma((groups,)),
            dma((groups,)),
            dma((6, 2)),
            dma((6, 2)),
            dma((6, max(groups, 4))),
            dma((6, max(groups, 4))),
        ],
        compiler_params=pltpu.CompilerParams(
            collective_id=1, has_side_effects=True, vmem_limit_bytes=62 << 20
        ),
        name="program",
    )(
        query_rows,
        key_rows,
        value_rows,
        key_bias,
        tri,
        mixer_weight,
        mixer_gain.reshape(1, width),
        routed_input,
        entry_gain.reshape(1, width),
        expert_index,
        route_weights,
        exit_gain.reshape(1, width),
        *weights,
    )


def solution(mesh):
    in_specs = (
        P("ep", "tp"),
        P("ep", "tp"),
        P("ep", "tp"),
        P("ep", "tp"),
        P("tp", None),
        P(),
        P(("ep", "tp"), None),
        P(),
        P(("ep", "tp"), None),
        P(("ep", "tp"), None),
        P("ep", None, "tp"),
        P("ep", None, "tp"),
        P("ep", "tp", None),
        P(None, "tp"),
        P(None, "tp"),
        P("tp", None),
        P(),
    )
    out_specs = (P(("ep", "tp"), None), P(("ep", "tp"), None))
    return jax.shard_map(
        on_device, mesh=mesh, in_specs=in_specs, out_specs=out_specs, check_vma=False
    )
```

```python
import functools

import jax
import jax.numpy as jnp
from jax import lax
from jax.experimental import pallas as pl
from jax.experimental.pallas import tpu as pltpu
from jax.sharding import PartitionSpec as P

EPS = 1e-06
PLANE = 8
CAPACITY = 2
NEAR = 1
RING_STEPS = (3, 5, 6, 7)


def root_norm(values, gain_row):
    return values * lax.rsqrt(jnp.mean(values * values, axis=-1, keepdims=True) + EPS) * gain_row


def stick_turn(query, blocks, biases, carry, tri, masks):
    keys = tri.shape[0]
    levels, weights = [], []
    for block, bias, mask in zip(blocks, biases, masks):
        score = (
            lax.dot_general(
                query, block, (((1,), (1,)), ((), ())), preferred_element_type=jnp.float32
            )
            + bias
        )
        fail = jnp.maximum(score, 0.0) + jnp.log(1.0 + jnp.exp(-jnp.abs(score)))
        counted = fail if mask is None else jnp.where(mask, fail, 0.0)
        sums = jnp.dot(counted.astype(jnp.bfloat16), tri, preferred_element_type=jnp.float32)
        total = jnp.broadcast_to(sums[:, 0:1] + counted[:, 0:1], carry.shape)
        levels.append(((score - fail) - sums, total))
    for (level, total), mask in zip(levels, masks):
        weight = jnp.exp(level - jnp.concatenate([carry] * (keys // carry.shape[1]), axis=1))
        if mask is not None:
            weight = jnp.where(mask, weight, 0.0)
        weights.append(weight.astype(jnp.bfloat16))
        carry = carry + total
    out = jnp.dot(
        jnp.concatenate(weights, axis=1),
        jnp.concatenate(blocks, axis=0),
        preferred_element_type=jnp.float32,
    )
    return out, carry


def silu_product(gate, up):
    return (gate / (1.0 + jnp.exp(-gate)) * up).astype(jnp.bfloat16)


def program_kernel(
    groups,
    plane,
    query_ref,
    key_ref,
    value_ref,
    bias_ref,
    mixer_hbm,
    mixer_gain_ref,
    input_ref,
    entry_gain_ref,
    index_ref,
    weight_ref,
    exit_gain_ref,
    gate_hbm,
    up_hbm,
    down_hbm,
    shared_gate_hbm,
    shared_up_hbm,
    shared_down_hbm,
    mixer_out,
    expert_out,
    normed,
    outgoing,
    back,
    stage,
    rows,
    partial,
    first_sum,
    second_sum,
    result,
    returned,
    neighbours,
    shared_part,
    shared_first,
    shared_second,
    kv_own,
    query_own,
    kv_all,
    queries,
    running,
    carried,
    far_part,
    attended_back,
    attended,
    mixer_part,
    mixer_first,
    mixer_second,
    mixer_w,
    gate_w,
    up_w,
    down_w,
    shared_gate_w,
    shared_up_w,
    shared_down_w,
    mixing_high,
    mixing_low,
    tri_ref,
    meta,
    near_out,
    near_stage,
    near_return,
    weight_sem,
    own_sem,
    z_send,
    z_recv,
    p_send,
    p_recv,
    x_send,
    x_recv,
    q_send,
    q_recv,
    b_send,
    b_recv,
    s_send,
    s_recv,
    a_send,
    a_recv,
    n_send,
    n_recv,
    m_send,
    m_recv,
):
    f32, bf16 = jnp.float32, jnp.bfloat16
    own_ep = lax.axis_index("ep")
    own_x = lax.axis_index("tp")
    own_z = own_ep // plane
    own_p = own_ep % plane
    own_y = own_p // 2
    own_core = own_p % 2
    lines = plane // 2
    half = plane // 2
    right = (own_x + 1) % 4
    left = (own_x + 3) % 4
    opposite = (own_x + 2) % 4
    side = (right, left)
    experts, width = gate_w.shape[0], gate_w.shape[1]
    shared_rows = normed.shape[0]
    shared_half = shared_rows // 2
    tokens = key_ref.shape[0]
    head_size = query_ref.shape[1] // lines
    mixer_rows = tokens // 4
    mixer_half = mixer_rows // 2
    block_slots = plane * experts * CAPACITY
    slots = groups * block_slots
    near = min(NEAR, groups)
    far = groups - near
    kept = 1
    summed = groups - kept

    def remote(src, dst, send_sem, recv_sem, ep, tp):
        return pltpu.make_async_remote_copy(
            src_ref=src,
            dst_ref=dst,
            send_sem=send_sem,
            recv_sem=recv_sem,
            device_id=(ep, tp),
            device_id_type=pl.DeviceIdType.MESH,
        )

    def offset(c):
        odd = c % 2
        return (odd * ((c + 1) // 2) + (1 - odd) * (groups - c // 2)) % groups

    def z_copy(c):
        there = (own_z + offset(c)) % groups
        return remote(
            outgoing.at[there], stage.at[c], z_send.at[0], z_recv.at[c], there * plane + own_p, own_x
        )

    def p_copy(c, i):
        there = (own_p + i) % plane
        return remote(
            stage.at[c, there],
            rows.at[0, c, own_p],
            p_send.at[0],
            p_recv.at[c],
            own_z * plane + there,
            own_x,
        )

    def p_own(c):
        return pltpu.make_async_copy(stage.at[c, own_p], rows.at[0, c, own_p], own_sem.at[c])

    def x_copy(c, way):
        return remote(
            rows.at[0, c], rows.at[1 + way, c], x_send.at[0], x_recv.at[0, c], own_ep, side[way]
        )

    def f_copy(c, way):
        part = pl.ds(way * half, half)
        return remote(
            rows.at[1 + way, c, part],
            rows.at[3, c, part],
            x_send.at[1],
            x_recv.at[1, c],
            own_ep,
            side[way],
        )

    def r_copy(c, way):
        return remote(
            partial.at[3, c, pl.ds(way * half, half)],
            first_sum.at[way, c],
            x_send.at[2],
            x_recv.at[2, c],
            own_ep,
            side[way],
        )

    def t_copy(c, way):
        return remote(
            partial.at[2 - way, c],
            second_sum.at[way, c],
            x_send.at[3],
            x_recv.at[3, c],
            own_ep,
            side[way],
        )

    def q_copy(c, i):
        there = (own_p + i) % plane
        return remote(
            result.at[c, there],
            returned.at[c, own_p],
            q_send.at[0],
            q_recv.at[c],
            own_z * plane + there,
            own_x,
        )

    def q_own(c):
        return pltpu.make_async_copy(result.at[c, own_p], returned.at[c, own_p], own_sem.at[groups + c])

    def b_copy(c):
        there = (own_z + groups - offset(c)) % groups
        return remote(
            returned.at[c], back.at[c - kept], b_send.at[0], b_recv.at[0], there * plane + own_p, own_x
        )

    def shared_copy(kind, way):
        part = pl.ds(way * shared_half, shared_half)
        src, dst = (
            (normed, neighbours.at[way]),
            (neighbours.at[way, part], neighbours.at[2, part]),
            (shared_part.at[3, part], shared_first.at[way]),
            (shared_part.at[2 - way], shared_second.at[way]),
        )[kind]
        return remote(src, dst, s_send.at[kind], s_recv.at[kind], own_ep, side[way])

    mirror = (groups - 1 - own_z) * plane + own_p
    partner = own_z * plane + own_p + 1 - 2 * own_core

    def k_copy(i):
        line = (own_y + i) % lines
        return remote(
            kv_own.at[line],
            kv_all.at[own_z, own_core, own_y],
            a_send.at[0],
            a_recv.at[0],
            own_z * plane + 2 * line + own_core,
            own_x,
        )

    def ask_copy(i):
        line = (own_y + i) % lines
        return remote(
            query_own.at[line],
            queries.at[own_y],
            a_send.at[1],
            a_recv.at[1],
            own_z * plane + 2 * line + own_core,
            own_x,
        )

    def ring_copy(way, r):
        source = (own_z + groups + (2 * way - 1) * r) % groups
        there = (own_z + groups + 1 - 2 * way) % groups
        block = kv_all.at[source, own_core]
        return remote(
            block, block, a_send.at[6], a_recv.at[6 + way * hops[0] + r], there * plane + own_p, own_x
        )

    def core_copy(way, r):
        source = (own_z + groups + (2 * way - 1) * (r + 1)) % groups
        block = kv_all.at[source, own_core]
        return remote(block, block, a_send.at[3], a_recv.at[3], partner, own_x)

    def core_own():
        block = kv_all.at[own_z, own_core]
        return remote(block, block, a_send.at[3], a_recv.at[3], partner, own_x)

    hops = ((groups - 1) // 2, groups // 2)
    others = pl.ds(0, plane - 1)
    outer = pl.ds(0, lines - 1)

    def meter(ref, send_sem, recv_sem):
        return remote(ref, ref, send_sem, recv_sem, own_ep, right)

    def arrived(ref, sem):
        meter(ref, sem, sem).wait_recv()

    def left_here(ref, sem):
        meter(ref, sem, sem).wait_send()

    shared_landing = (
        neighbours.at[pl.ds(0, 2)],
        neighbours.at[2],
        shared_first,
        shared_second,
        mixer_first,
        mixer_second,
    )

    def shared_arrived(kind):
        arrived(shared_landing[kind], s_recv.at[kind])

    def x_arrived(kind, c):
        landing = (
            rows.at[pl.ds(1, 2), c],
            rows.at[3, c],
            first_sum.at[:, c],
            second_sum.at[:, c],
        )[kind]
        arrived(landing, x_recv.at[kind, c])

    def p_arrived(c):
        arrived(rows.at[0, c, others], p_recv.at[c])
        p_own(c).wait()

    def near_arrived(c):
        arrived(rows.at[pl.ds(1, 3), c, others], n_recv.at[3 + c])
        near_p_own(c).wait()

    def q_arrived(c):
        arrived(returned.at[c, others], q_recv.at[c])
        q_own(c).wait()


    def meta_copy(way):
        return remote(
            meta.at[0], meta.at[1 + way], m_send.at[0], m_recv.at[0], own_ep, side[way]
        )

    meta_far = remote(meta.at[1], meta.at[3], m_send.at[0], m_recv.at[1], own_ep, right)

    def near_z(c):
        there = (own_z + offset(c)) % groups
        return remote(
            near_out.at[c],
            near_stage.at[c - 1],
            n_send.at[0],
            n_recv.at[c],
            there * plane + own_p,
            own_x,
        )

    def near_source(c, place):
        return near_out.at[0, place] if c == 0 else near_stage.at[c - 1, place]

    def near_p(c, i):
        there = (own_p + i) % plane
        return remote(
            near_source(c, there),
            rows.at[pl.ds(1, 3), c, own_p],
            n_send.at[1],
            n_recv.at[3 + c],
            own_z * plane + there,
            own_x,
        )

    def near_p_own(c):
        return pltpu.make_async_copy(
            near_source(c, own_p), rows.at[pl.ds(1, 3), c, own_p], own_sem.at[2 * groups + 4 + c]
        )

    def near_q(c, i):
        there = (own_p + i) % plane
        return remote(
            partial.at[:, c, there],
            near_return.at[c, own_p],
            n_send.at[2],
            n_recv.at[6],
            own_z * plane + there,
            own_x,
        )

    def near_q_own(c):
        return pltpu.make_async_copy(
            partial.at[:, c, own_p], near_return.at[c, own_p], own_sem.at[2 * groups + 7]
        )

    def answer_copy(i):
        line = (own_y + i) % lines
        return remote(
            attended_back.at[line],
            attended.at[own_y],
            a_send.at[2],
            a_recv.at[2],
            own_z * plane + 2 * line + own_core,
            own_x,
        )

    ask_far = remote(
        queries.at[pl.ds(2, 2)], queries.at[pl.ds(4, 2)], a_send.at[4], a_recv.at[4], mirror, own_x
    )
    answer_far = remote(
        far_part, attended_back.at[pl.ds(2, 2)], a_send.at[5], a_recv.at[5], mirror, own_x
    )
    k_own = pltpu.make_async_copy(
        kv_own.at[own_y], kv_all.at[own_z, own_core, own_y], own_sem.at[2 * groups + 1]
    )
    ask_own = pltpu.make_async_copy(query_own.at[own_y], queries.at[own_y], own_sem.at[2 * groups + 2])
    answer_own = pltpu.make_async_copy(
        attended_back.at[own_y], attended.at[own_y], own_sem.at[2 * groups + 3]
    )

    def mixer_copy(kind, way):
        part = pl.ds(way * mixer_half, mixer_half)
        src, dst = (
            (mixer_part.at[opposite, part], mixer_first.at[way]),
            (mixer_part.at[side[way]], mixer_second.at[way]),
        )[kind]
        return remote(src, dst, s_send.at[4 + kind], s_recv.at[4 + kind], own_ep, side[way])

    first_z = pltpu.make_async_copy(outgoing.at[own_z], stage.at[0], own_sem.at[2 * groups])
    loads = [
        pltpu.make_async_copy(src, dst, weight_sem.at[n])
        for n, (src, dst) in enumerate(
            (
                (shared_gate_hbm, shared_gate_w),
                (shared_up_hbm, shared_up_w),
                (shared_down_hbm, shared_down_w),
                (gate_hbm, gate_w),
                (up_hbm, up_w),
                (down_hbm, down_w),
                (mixer_hbm, mixer_w),
            )
        )
    ]

    barrier = pltpu.get_barrier_semaphore()

    def greet(ep, tp):
        pl.semaphore_signal(
            barrier, inc=1, device_id=(ep, tp), device_id_type=pl.DeviceIdType.MESH
        )

    for k in range(1, groups):
        greet(((own_z + k) % groups) * plane + own_p, own_x)
    for k in range(1, plane):
        greet(own_z * plane + (own_p + k) % plane, own_x)
    greet(own_ep, right)
    greet(own_ep, left)
    for load in loads:
        load.start()

    normed[...] = root_norm(input_ref[...].astype(f32), entry_gain_ref[...]).astype(bf16)

    lane = lax.broadcasted_iota(jnp.int32, (tokens, 128), 1)
    low = lane < head_size
    bias_rows = bias_ref[...].astype(f32)
    tri_row = lax.broadcasted_iota(jnp.int32, tri_ref.shape, 0)
    tri_column = lax.broadcasted_iota(jnp.int32, tri_ref.shape, 1)
    tri_ref[...] = jnp.where(tri_row > tri_column, 1.0, 0.0).astype(bf16)
    for head in range(lines):
        column = (head // 2) * 128

        def placed(ref, upper):
            group = ref[:, column : column + 128].astype(f32)
            return group if head % 2 == upper else pltpu.roll(group, head_size, 1)

        kv_own[head, :tokens] = jnp.where(low, placed(key_ref, 0), placed(value_ref, 1)).astype(bf16)
        kv_own[head, tokens:] = jnp.broadcast_to(bias_rows[head : head + 1], (16, 128)).astype(bf16)
        query_own[head] = jnp.where(low, placed(query_ref, 0) * head_size**-0.5, 0.0).astype(bf16)

    expert_row = lax.broadcasted_iota(jnp.int32, (slots // CAPACITY, shared_rows), 0)
    named = [(expert_row == index_ref[k : k + 1]).astype(f32) for k in range(2)]
    earlier = (
        lax.broadcasted_iota(jnp.int32, (shared_rows, shared_rows), 0)
        < lax.broadcasted_iota(jnp.int32, (shared_rows, shared_rows), 1)
    ).astype(f32).astype(bf16)
    before = jnp.dot((named[0] + named[1]).astype(bf16), earlier, preferred_element_type=f32)
    meta[0] = jnp.zeros((8, 128), f32)
    for k in range(2):
        rank = jnp.sum(named[k] * before, axis=0, keepdims=True)
        meta[0, k : k + 1, :shared_rows] = index_ref[k : k + 1].astype(f32) * CAPACITY + rank
        meta[0, 2 + k : 3 + k, :shared_rows] = weight_ref[k : k + 1]

    def slot_hits(j, first, count):
        number = (lax.broadcasted_iota(jnp.int32, (count, shared_rows), 0) + first).astype(f32)
        return [number == meta[j, k : k + 1, :shared_rows] for k in range(2)]

    def picked(j, first, count):
        hits = slot_hits(j, first, count)
        return (hits[0] | hits[1]).astype(f32).astype(bf16)

    def weighted(j, first, count):
        hits = slot_hits(j, first, count)
        return jnp.where(hits[0], meta[j, 2:3, :shared_rows], 0.0) + jnp.where(
            hits[1], meta[j, 3:4, :shared_rows], 0.0
        )

    def chunk_first(c):
        return ((own_z + offset(c)) % groups) * block_slots

    def halves(value):
        high = value.astype(bf16)
        return high, (value - high.astype(f32)).astype(bf16)

    outgoing[...] = (
        jnp.dot(picked(0, 0, slots), normed[...], preferred_element_type=f32)
        .astype(bf16)
        .reshape(outgoing.shape)
    )
    for c in range(kept, groups):
        part = slice((c - kept) * block_slots, (c - kept + 1) * block_slots)
        mixing_high[part], mixing_low[part] = halves(weighted(0, chunk_first(c), block_slots))
    running[...] = jnp.zeros_like(running)
    carried[...] = jnp.zeros_like(carried)
    first_z.start()
    k_own.start()
    ask_own.start()
    pl.semaphore_wait(barrier, groups + plane)

    for way in range(2):
        shared_copy(0, way).start()
        meta_copy(way).start()
    for c in range(near, min(groups, near + 4)):
        z_copy(c).start()
    for i in range(1, lines):
        k_copy(i).start()
        ask_copy(i).start()
    first_z.wait()

    def compute_shared():
        def one_block(source, target):
            block = source[...]
            gate = jnp.dot(block, shared_gate_w[...], preferred_element_type=f32)
            up = jnp.dot(block, shared_up_w[...], preferred_element_type=f32)
            hidden = silu_product(gate, up)
            target[...] = jnp.dot(hidden, shared_down_w[...], preferred_element_type=f32).astype(bf16)

        one_block(normed, shared_part.at[0])
        for j in range(3):
            one_block(neighbours.at[j], shared_part.at[j + 1])

    def compute_rows(c):
        count = 4 * plane * CAPACITY
        for e in range(experts):
            block = rows[:, c, :, e].reshape(count, width)
            gate = jnp.dot(block, gate_w[e], preferred_element_type=f32)
            up = jnp.dot(block, up_w[e], preferred_element_type=f32)
            hidden = silu_product(gate, up)
            product = jnp.dot(hidden, down_w[e], preferred_element_type=f32).astype(bf16)
            partial[:, c, :, e] = product.reshape(4, plane, CAPACITY, width)

    def flat(value):
        return value.reshape(-1, width).astype(f32)

    def add_first(c):
        for way in range(2):
            part = pl.ds(way * half, half)
            total = flat(partial[2 - way, c, part]) + flat(first_sum[way, c])
            partial[2 - way, c, part] = total.astype(bf16).reshape(half, experts, CAPACITY, width)

    def add_second(c):
        total = flat(partial[0, c]) + flat(second_sum[0, c]) + flat(second_sum[1, c])
        result[c] = total.astype(bf16).reshape(plane, experts, CAPACITY, width)

    def gather_near():
        for j in range(1, 4):
            picks = jnp.concatenate([picked(j, chunk_first(c), block_slots) for c in range(near)], axis=0)
            chosen = jnp.dot(picks, neighbours[j - 1], preferred_element_type=f32).astype(bf16)
            near_out[:, :, j - 1] = chosen.reshape(near, plane, experts, CAPACITY, width)

    def combine_near():
        for j in range(4):
            mixing = weighted(j, chunk_first(0), block_slots)
            found = near_return[0, :, j].reshape(block_slots, width)
            total = shared_part[j].astype(f32)
            for piece in halves(mixing):
                total += lax.dot_general(
                    piece, found, (((0,), (0,)), ((), ())), preferred_element_type=f32
                )
            shared_part[j] = total.astype(bf16)

    first_turns = own_z + 1
    turns = groups + 1
    share = (turns + 2) // 3

    def attend_turn(turn, unused):
        second = jnp.where(turn >= first_turns, 1, 0)
        query_z = own_z + second * (groups - 1 - 2 * own_z)
        key_z = query_z - (turn - second * first_turns)

        def run(masked):
            query = queries[pl.ds(4 * second, 2)].reshape(2 * tokens, 128)
            blocks, biases, masks = [], [], []
            for line in range(lines - 1, -1, -1):
                pair = [kv_all[key_z, core, line] for core in range(2)]
                blocks.append(jnp.concatenate([b[:tokens] for b in pair], axis=0))
                biases.append(
                    jnp.concatenate([b[tokens:][:1] for b in pair], axis=1).astype(f32)
                )
                if masked:
                    row = lax.broadcasted_iota(jnp.int32, (2 * tokens, 2 * tokens), 0)
                    column = lax.broadcasted_iota(jnp.int32, (2 * tokens, 2 * tokens), 1)
                    limit = (2 * second - line) * 2 * tokens + own_core * tokens
                    masks.append(column - (row + (row // tokens) * tokens) < limit)
                else:
                    masks.append(None)
            out, carry = stick_turn(query, blocks, biases, carried[second], tri_ref[...], masks)
            running[second] = running[second] + out
            carried[second] = carry

        @pl.when(key_z == query_z)
        def _():
            run(True)

        @pl.when(key_z != query_z)
        def _():
            run(False)

        return unused

    def finish_attention():
        low2 = lax.broadcasted_iota(jnp.int32, (2 * tokens, 128), 1) < head_size
        even = own_y % 2 == 0
        for second, target in ((0, attended_back.at[pl.ds(0, 2)]), (1, far_part)):
            value = running[second]
            value = jnp.where(even, pltpu.roll(value, head_size, 1), value)
            target[...] = value.astype(bf16).reshape(2, tokens, 128)

    def mix():
        low1 = lax.broadcasted_iota(jnp.int32, (tokens, 128), 1) < head_size
        groups_of_two = [
            jnp.where(low1, attended[2 * n].astype(f32), attended[2 * n + 1].astype(f32)).astype(bf16)
            for n in range(lines // 2)
        ]
        gathered = jnp.concatenate(groups_of_two, axis=1)
        product = jnp.dot(gathered, mixer_w[...], preferred_element_type=f32).astype(bf16)
        mixer_part[...] = product.reshape(4, mixer_rows, width)

    def chunk(i):
        return i + near - (i // max(far, 1)) * summed

    def step(s, unused):
        @pl.when(s == 12)
        def _():
            answer_far.wait_recv()
            answer_own.start()
            for i in range(1, lines):
                answer_copy(i).start()

        @pl.when(s < far)
        def _():
            c = s + near
            z_copy(c).wait_recv()
            p_own(c).start()
            for i in range(1, plane):
                p_copy(c, i).start()

        @pl.when(s == 1)
        def _():
            arrived(kv_all.at[own_z, own_core, outer], a_recv.at[0])
            k_own.wait()
            for way in range(2):
                if hops[way] > 0:
                    ring_copy(way, 0).start()
            core_own().start()
            for c in range(near + 4, groups):
                z_copy(c).start()
            arrived(queries.at[outer], a_recv.at[1])
            ask_own.wait()
            ask_far.start()

        @pl.when(s == 2)
        def _():
            shared_arrived(0)
            arrived(meta.at[pl.ds(1, 2)], m_recv.at[0])
            for way in range(2):
                shared_copy(1, way).start()
            meta_far.start()

        @pl.when((s >= 1) & (s < far + 1))
        def _():
            c = s - 1 + near
            p_arrived(c)
            for way in range(2):
                x_copy(c, way).start()

        @pl.when((s >= 2) & (s < far + 2))
        def _():
            c = s - 2 + near
            x_arrived(0, c)
            for way in range(2):
                f_copy(c, way).start()

        for r in range(hops[1]):

            @pl.when(s == RING_STEPS[r])
            def _():
                for way in range(2):
                    if r < hops[way]:
                        ring_copy(way, r).wait_recv()
                        if r + 1 < hops[way]:
                            ring_copy(way, r + 1).start()
                        core_copy(way, r).start()

        @pl.when(s == 3)
        def _():
            shared_arrived(1)
            meta_far.wait_recv()
            gather_near()
            for c in range(1, near):
                near_z(c).start()
                z_copy(c).start()
            p_own(0).start()
            near_p_own(0).start()
            for i in range(1, plane):
                p_copy(0, i).start()
                near_p(0, i).start()

        @pl.when(s == 4)
        def _():
            for load in loads:
                load.wait()

        @pl.when((s >= 4) & (s < far + 4))
        def _():
            c = s - 4 + near
            x_arrived(1, c)
            compute_rows(c)
            for way in range(2):
                r_copy(c, way).start()

        @pl.when(s == 6)
        def _():
            p_arrived(0)
            near_arrived(0)
            compute_rows(0)
            near_q_own(0).start()
            for i in range(1, plane):
                near_q(0, i).start()

        for c in range(1, near):

            @pl.when(s == far + 3 + c)
            def _():
                p_arrived(c)
                near_arrived(c)
                compute_rows(c)
                for way in range(2):
                    r_copy(c, way).start()

        @pl.when((s >= 5) & (s < summed + 5))
        def _():
            c = chunk(s - 5)
            x_arrived(2, c)
            add_first(c)
            for way in range(2):
                t_copy(c, way).start()

        @pl.when((s >= 6) & (s < summed + 6))
        def _():
            c = chunk(s - 6)
            x_arrived(3, c)
            add_second(c)
            q_own(c).start()
            for i in range(1, plane):
                q_copy(c, i).start()

        @pl.when((s >= 8) & (s < summed + 8))
        def _():
            c = chunk(s - 8)
            q_arrived(c)
            b_copy(c).start()

        @pl.when(s == 5)
        def _():
            compute_shared()

        if near > 1:

            @pl.when(s == 7)
            def _():
                for c in range(1, near):
                    near_z(c).wait_recv()
                    z_copy(c).wait_recv()
                    p_own(c).start()
                    near_p_own(c).start()
                    for i in range(1, plane):
                        p_copy(c, i).start()
                        near_p(c, i).start()

        @pl.when(s == 8)
        def _():
            arrived(kv_all.at[:, 0], a_recv.at[3])
            ask_far.wait_recv()

        @pl.when((s >= 8) & (s < 11))
        def _():
            first = (s - 8) * share
            lax.fori_loop(first, jnp.minimum(first + share, turns), attend_turn, 0)

        @pl.when(s == 10)
        def _():
            finish_attention()
            answer_far.start()
            arrived(near_return.at[0, others], n_recv.at[6])
            near_q_own(0).wait()
            combine_near()

        @pl.when(s == 11)
        def _():
            for way in range(2):
                shared_copy(2, way).start()

        @pl.when(s == 12)
        def _():
            arrived(attended.at[outer], a_recv.at[2])
            answer_own.wait()
            mix()
            for way in range(2):
                mixer_copy(0, way).start()
            shared_arrived(2)
            for way in range(2):
                part = pl.ds(way * shared_half, shared_half)
                shared_part[2 - way, part] = (
                    shared_part[2 - way, part].astype(f32) + shared_first[way].astype(f32)
                ).astype(bf16)
                shared_copy(3, way).start()

        @pl.when(s == 13)
        def _():
            shared_arrived(4)
            for way in range(2):
                part = pl.ds(way * mixer_half, mixer_half)
                mixer_part[side[way], part] = (
                    mixer_part[side[way], part].astype(f32) + mixer_first[way].astype(f32)
                ).astype(bf16)
                mixer_copy(1, way).start()

        return unused

    lax.fori_loop(0, max(summed + 8, 14), step, 0)

    shared_arrived(5)
    mixer_out[...] = root_norm(
        mixer_part[own_x].astype(f32) + mixer_second[0].astype(f32) + mixer_second[1].astype(f32),
        mixer_gain_ref[...],
    ).astype(bf16)
    arrived(back, b_recv.at[0])
    rows_back = back[...].reshape(summed * block_slots, width)
    combined = sum(
        lax.dot_general(m[...], rows_back, (((0,), (0,)), ((), ())), preferred_element_type=f32)
        for m in (mixing_high, mixing_low)
    )
    shared_arrived(3)
    combined = (
        combined
        + shared_part[0].astype(f32)
        + shared_second[0].astype(f32)
        + shared_second[1].astype(f32)
    )
    expert_out[...] = root_norm(combined, exit_gain_ref[...]).astype(bf16)

    for ref, sem in (
        (stage.at[pl.ds(0, groups - 1)], z_send.at[0]),
        (stage.at[:, others], p_send.at[0]),
        (rows.at[pl.ds(0, 2), pl.ds(0, far)], x_send.at[0]),
        (rows.at[0, pl.ds(0, far)], x_send.at[1]),
        (partial.at[0, pl.ds(0, summed)], x_send.at[2]),
        (partial.at[pl.ds(0, 2), pl.ds(0, summed)], x_send.at[3]),
        (returned.at[pl.ds(0, summed), others], q_send.at[0]),
        (returned.at[pl.ds(0, summed)], b_send.at[0]),
        (meta.at[pl.ds(1, 3)], m_send.at[0]),
        (kv_all.at[own_z, own_core, outer], a_send.at[0]),
        (queries.at[outer], a_send.at[1]),
        (attended.at[outer], a_send.at[2]),
        (kv_all.at[:, 0], a_send.at[3]),
        (kv_all.at[pl.ds(0, groups - 1), 0], a_send.at[6]),
        (near_out.at[:, others], n_send.at[1]),
        (near_return.at[0, others], n_send.at[2]),
    ):
        left_here(ref, sem)
    if near > 1:
        left_here(near_stage.at[pl.ds(0, near - 1)], n_send.at[0])
    for kind, ref in enumerate(shared_landing):
        left_here(ref, s_send.at[kind])
    ask_far.wait_send()
    answer_far.wait_send()


def on_device(
    query_rows,
    key_rows,
    value_rows,
    key_bias,
    mixer_weight,
    mixer_gain,
    routed_input,
    entry_gain,
    expert_index,
    route_weights,
    expert_gate,
    expert_up,
    expert_down,
    shared_gate,
    shared_up,
    shared_down,
    exit_gain,
):
    bf16, f32 = jnp.bfloat16, jnp.float32
    plane = PLANE
    groups = lax.axis_size("ep") // plane
    lines, half = plane // 2, plane // 2
    tokens = query_rows.shape[0]
    count, width = routed_input.shape
    experts = expert_gate.shape[0]
    block = (plane, experts, CAPACITY, width)
    near = min(NEAR, groups)
    kept_slots = (groups - 1) * plane * experts * CAPACITY
    vmem = pl.BlockSpec(memory_space=pltpu.VMEM)
    hbm = pl.BlockSpec(memory_space=pl.ANY)
    weights = (expert_gate, expert_up, expert_down, shared_gate, shared_up, shared_down)
    dma = pltpu.SemaphoreType.DMA
    return pl.pallas_call(
        functools.partial(program_kernel, groups, plane),
        out_shape=(
            jax.ShapeDtypeStruct((tokens // 4, width), bf16),
            jax.ShapeDtypeStruct((count, width), bf16),
        ),
        in_specs=[vmem] * 4 + [hbm] + [vmem] * 6 + [hbm] * 6,
        out_specs=(vmem, vmem),
        scratch_shapes=[
            pltpu.VMEM((count, width), bf16),
            pltpu.VMEM((groups,) + block, bf16),
            pltpu.VMEM((groups - 1,) + block, bf16),
            pltpu.VMEM((groups,) + block, bf16),
            pltpu.VMEM((4, groups) + block, bf16),
            pltpu.VMEM((4, groups) + block, bf16),
            pltpu.VMEM((2, groups, half) + block[1:], bf16),
            pltpu.VMEM((2, groups) + block, bf16),
            pltpu.VMEM((groups,) + block, bf16),
            pltpu.VMEM((groups,) + block, bf16),
            pltpu.VMEM((3, count, width), bf16),
            pltpu.VMEM((4, count, width), bf16),
            pltpu.VMEM((2, count // 2, width), bf16),
            pltpu.VMEM((2, count, width), bf16),
            pltpu.VMEM((lines, tokens + 16, 128), bf16),
            pltpu.VMEM((lines, tokens, 128), bf16),
            pltpu.VMEM((groups, 2, lines, tokens + 16, 128), bf16),
            pltpu.VMEM((6, tokens, 128), bf16),
            pltpu.VMEM((2, 2 * tokens, 128), f32),
            pltpu.VMEM((2, 2 * tokens, 128), f32),
            pltpu.VMEM((2, tokens, 128), bf16),
            pltpu.VMEM((lines, tokens, 128), bf16),
            pltpu.VMEM((lines, tokens, 128), bf16),
            pltpu.VMEM((4, tokens // 4, width), bf16),
            pltpu.VMEM((2, tokens // 8, width), bf16),
            pltpu.VMEM((2, tokens // 4, width), bf16),
            pltpu.VMEM(mixer_weight.shape, bf16),
        ]
        + [pltpu.VMEM(w.shape, bf16) for w in weights]
        + [
            pltpu.VMEM((kept_slots, count), bf16),
            pltpu.VMEM((kept_slots, count), bf16),
            pltpu.VMEM((2 * tokens, 2 * tokens), bf16),
            pltpu.VMEM((4, 8, 128), f32),
            pltpu.VMEM((near, plane, 3) + block[1:], bf16),
            pltpu.VMEM((max(near - 1, 1), plane, 3) + block[1:], bf16),
            pltpu.VMEM((1, plane, 4) + block[1:], bf16),
            dma((7,)),
            dma((2 * groups + 8,)),
            dma((1,)),
            dma((groups,)),
            dma((1,)),
            dma((groups,)),
            dma((4,)),
            dma((4, groups)),
            dma((1,)),
            dma((groups,)),
            dma((1,)),
            dma((1,)),
            dma((6,)),
            dma((6,)),
            dma((7,)),
            dma((6 + groups,)),
            dma((3,)),
            dma((7,)),
            dma((1,)),
            dma((2,)),
        ],
        compiler_params=pltpu.CompilerParams(
            collective_id=1, has_side_effects=True, vmem_limit_bytes=62 << 20
        ),
        name="program",
    )(
        query_rows,
        key_rows,
        value_rows,
        jnp.transpose(key_bias),
        mixer_weight,
        mixer_gain.reshape(1, width),
        routed_input,
        entry_gain.reshape(1, width),
        jnp.transpose(expert_index),
        jnp.transpose(route_weights),
        exit_gain.reshape(1, width),
        *weights,
    )


def solution(mesh):
    in_specs = (
        P("ep", "tp"),
        P("ep", "tp"),
        P("ep", "tp"),
        P("ep", "tp"),
        P("tp", None),
        P(),
        P(("ep", "tp"), None),
        P(),
        P(("ep", "tp"), None),
        P(("ep", "tp"), None),
        P("ep", None, "tp"),
        P("ep", None, "tp"),
        P("ep", "tp", None),
        P(None, "tp"),
        P(None, "tp"),
        P("tp", None),
        P(),
    )
    out_specs = (P(("ep", "tp"), None), P(("ep", "tp"), None))
    return jax.shard_map(
        on_device, mesh=mesh, in_specs=in_specs, out_specs=out_specs, check_vma=False
    )
```

```python
import functools

import jax
import jax.numpy as jnp
from jax import lax
from jax.experimental import pallas as pl
from jax.experimental.pallas import tpu as pltpu
from jax.sharding import PartitionSpec as P

EPS = 1e-06
PLANE = 8
CAPACITY = 2
NEAR = 2
RING_STEPS = (3, 5, 6, 7)


def root_norm(values, gain_row):
    return values * lax.rsqrt(jnp.mean(values * values, axis=-1, keepdims=True) + EPS) * gain_row


def stick_turn(query, blocks, biases, carry, tri, masks):
    keys = tri.shape[0]
    levels, weights = [], []
    for block, bias, mask in zip(blocks, biases, masks):
        score = (
            lax.dot_general(
                query, block, (((1,), (1,)), ((), ())), preferred_element_type=jnp.float32
            )
            + bias
        )
        fail = jnp.maximum(score, 0.0) + jnp.log(1.0 + jnp.exp(-jnp.abs(score)))
        counted = fail if mask is None else jnp.where(mask, fail, 0.0)
        sums = jnp.dot(counted.astype(jnp.bfloat16), tri, preferred_element_type=jnp.float32)
        total = jnp.broadcast_to(sums[:, 0:1] + counted[:, 0:1], carry.shape)
        levels.append(((score - fail) - sums, total))
    for (level, total), mask in zip(levels, masks):
        weight = jnp.exp(level - jnp.concatenate([carry] * (keys // carry.shape[1]), axis=1))
        if mask is not None:
            weight = jnp.where(mask, weight, 0.0)
        weights.append(weight.astype(jnp.bfloat16))
        carry = carry + total
    out = jnp.dot(
        jnp.concatenate(weights, axis=1),
        jnp.concatenate(blocks, axis=0),
        preferred_element_type=jnp.float32,
    )
    return out, carry


def silu_product(gate, up):
    return (gate / (1.0 + jnp.exp(-gate)) * up).astype(jnp.bfloat16)


def program_kernel(
    groups,
    plane,
    query_ref,
    key_ref,
    value_ref,
    bias_ref,
    mixer_hbm,
    mixer_gain_ref,
    input_ref,
    entry_gain_ref,
    index_ref,
    weight_ref,
    exit_gain_ref,
    gate_hbm,
    up_hbm,
    down_hbm,
    shared_gate_hbm,
    shared_up_hbm,
    shared_down_hbm,
    mixer_out,
    expert_out,
    normed,
    outgoing,
    back,
    stage,
    rows,
    partial,
    first_sum,
    second_sum,
    result,
    returned,
    neighbours,
    shared_part,
    shared_first,
    shared_second,
    kv_own,
    query_own,
    kv_all,
    queries,
    running,
    carried,
    far_part,
    attended_back,
    attended,
    mixer_part,
    mixer_first,
    mixer_second,
    mixer_w,
    gate_w,
    up_w,
    down_w,
    shared_gate_w,
    shared_up_w,
    shared_down_w,
    mixing_high,
    mixing_low,
    tri_ref,
    meta,
    near_out,
    near_stage,
    near_return,
    weight_sem,
    own_sem,
    z_send,
    z_recv,
    p_send,
    p_recv,
    x_send,
    x_recv,
    q_send,
    q_recv,
    b_send,
    b_recv,
    s_send,
    s_recv,
    a_send,
    a_recv,
    n_send,
    n_recv,
    m_send,
    m_recv,
):
    f32, bf16 = jnp.float32, jnp.bfloat16
    own_ep = lax.axis_index("ep")
    own_x = lax.axis_index("tp")
    own_z = own_ep // plane
    own_p = own_ep % plane
    own_y = own_p // 2
    own_core = own_p % 2
    lines = plane // 2
    half = plane // 2
    right = (own_x + 1) % 4
    left = (own_x + 3) % 4
    opposite = (own_x + 2) % 4
    side = (right, left)
    experts, width = gate_w.shape[0], gate_w.shape[1]
    shared_rows = normed.shape[0]
    shared_half = shared_rows // 2
    tokens = key_ref.shape[0]
    head_size = query_ref.shape[1] // lines
    mixer_rows = tokens // 4
    mixer_half = mixer_rows // 2
    block_slots = plane * experts * CAPACITY
    slots = groups * block_slots
    near = min(NEAR, groups)
    far = groups - near
    kept = 1
    summed = groups - kept

    def remote(src, dst, send_sem, recv_sem, ep, tp):
        return pltpu.make_async_remote_copy(
            src_ref=src,
            dst_ref=dst,
            send_sem=send_sem,
            recv_sem=recv_sem,
            device_id=(ep, tp),
            device_id_type=pl.DeviceIdType.MESH,
        )

    def offset(c):
        odd = c % 2
        return (odd * (groups - (c + 1) // 2) + (1 - odd) * (c // 2)) % groups

    def z_copy(c):
        there = (own_z + offset(c)) % groups
        return remote(
            outgoing.at[there], stage.at[c], z_send.at[0], z_recv.at[c], there * plane + own_p, own_x
        )

    def p_copy(c, i):
        there = (own_p + i) % plane
        return remote(
            stage.at[c, there],
            rows.at[0, c, own_p],
            p_send.at[0],
            p_recv.at[c],
            own_z * plane + there,
            own_x,
        )

    def p_own(c):
        return pltpu.make_async_copy(stage.at[c, own_p], rows.at[0, c, own_p], own_sem.at[c])

    def x_copy(c, way):
        return remote(
            rows.at[0, c], rows.at[1 + way, c], x_send.at[0], x_recv.at[0, c], own_ep, side[way]
        )

    def f_copy(c, way):
        part = pl.ds(way * half, half)
        return remote(
            rows.at[1 + way, c, part],
            rows.at[3, c, part],
            x_send.at[1],
            x_recv.at[1, c],
            own_ep,
            side[way],
        )

    def r_copy(c, way):
        return remote(
            partial.at[3, c, pl.ds(way * half, half)],
            first_sum.at[way, c],
            x_send.at[2],
            x_recv.at[2, c],
            own_ep,
            side[way],
        )

    def t_copy(c, way):
        return remote(
            partial.at[2 - way, c],
            second_sum.at[way, c],
            x_send.at[3],
            x_recv.at[3, c],
            own_ep,
            side[way],
        )

    def q_copy(c, i):
        there = (own_p + i) % plane
        return remote(
            result.at[c, there],
            returned.at[c, own_p],
            q_send.at[0],
            q_recv.at[c],
            own_z * plane + there,
            own_x,
        )

    def q_own(c):
        return pltpu.make_async_copy(result.at[c, own_p], returned.at[c, own_p], own_sem.at[groups + c])

    def b_copy(c):
        there = (own_z + groups - offset(c)) % groups
        return remote(
            returned.at[c], back.at[c - kept], b_send.at[0], b_recv.at[0], there * plane + own_p, own_x
        )

    def shared_copy(kind, way):
        part = pl.ds(way * shared_half, shared_half)
        src, dst = (
            (normed, neighbours.at[way]),
            (neighbours.at[way, part], neighbours.at[2, part]),
            (shared_part.at[3, part], shared_first.at[way]),
            (shared_part.at[2 - way], shared_second.at[way]),
        )[kind]
        return remote(src, dst, s_send.at[kind], s_recv.at[kind], own_ep, side[way])

    mirror = (groups - 1 - own_z) * plane + own_p
    partner = own_z * plane + own_p + 1 - 2 * own_core

    def k_copy(i):
        line = (own_y + i) % lines
        return remote(
            kv_own.at[line],
            kv_all.at[own_z, own_core, own_y],
            a_send.at[0],
            a_recv.at[0],
            own_z * plane + 2 * line + own_core,
            own_x,
        )

    def ask_copy(i):
        line = (own_y + i) % lines
        return remote(
            query_own.at[line],
            queries.at[own_y],
            a_send.at[1],
            a_recv.at[1],
            own_z * plane + 2 * line + own_core,
            own_x,
        )

    def ring_copy(way, r):
        source = (own_z + groups + (2 * way - 1) * r) % groups
        there = (own_z + groups + 1 - 2 * way) % groups
        block = kv_all.at[source, own_core]
        return remote(
            block, block, a_send.at[6], a_recv.at[6 + way * hops[0] + r], there * plane + own_p, own_x
        )

    def core_copy(way, r):
        source = (own_z + groups + (2 * way - 1) * (r + 1)) % groups
        block = kv_all.at[source, own_core]
        return remote(block, block, a_send.at[3], a_recv.at[3], partner, own_x)

    def core_own():
        block = kv_all.at[own_z, own_core]
        return remote(block, block, a_send.at[3], a_recv.at[3], partner, own_x)

    hops = ((groups - 1) // 2, groups // 2)
    others = pl.ds(0, plane - 1)
    outer = pl.ds(0, lines - 1)

    def meter(ref, send_sem, recv_sem):
        return remote(ref, ref, send_sem, recv_sem, own_ep, right)

    def arrived(ref, sem):
        meter(ref, sem, sem).wait_recv()

    def left_here(ref, sem):
        meter(ref, sem, sem).wait_send()

    shared_landing = (
        neighbours.at[pl.ds(0, 2)],
        neighbours.at[2],
        shared_first,
        shared_second,
        mixer_first,
        mixer_second,
    )

    def shared_arrived(kind):
        arrived(shared_landing[kind], s_recv.at[kind])

    def x_arrived(kind, c):
        landing = (
            rows.at[pl.ds(1, 2), c],
            rows.at[3, c],
            first_sum.at[:, c],
            second_sum.at[:, c],
        )[kind]
        arrived(landing, x_recv.at[kind, c])

    def p_arrived(c):
        arrived(rows.at[0, c, others], p_recv.at[c])
        p_own(c).wait()

    def near_arrived(c):
        arrived(rows.at[pl.ds(1, 3), c, others], n_recv.at[3 + c])
        near_p_own(c).wait()

    def q_arrived(c):
        arrived(returned.at[c, others], q_recv.at[c])
        q_own(c).wait()


    def meta_copy(way):
        return remote(
            meta.at[0], meta.at[1 + way], m_send.at[0], m_recv.at[0], own_ep, side[way]
        )

    meta_far = remote(meta.at[1], meta.at[3], m_send.at[0], m_recv.at[1], own_ep, right)

    def near_z(c):
        there = (own_z + offset(c)) % groups
        return remote(
            near_out.at[c],
            near_stage.at[c - 1],
            n_send.at[0],
            n_recv.at[c],
            there * plane + own_p,
            own_x,
        )

    def near_source(c, place):
        return near_out.at[0, place] if c == 0 else near_stage.at[c - 1, place]

    def near_p(c, i):
        there = (own_p + i) % plane
        return remote(
            near_source(c, there),
            rows.at[pl.ds(1, 3), c, own_p],
            n_send.at[1],
            n_recv.at[3 + c],
            own_z * plane + there,
            own_x,
        )

    def near_p_own(c):
        return pltpu.make_async_copy(
            near_source(c, own_p), rows.at[pl.ds(1, 3), c, own_p], own_sem.at[2 * groups + 4 + c]
        )

    def near_q(c, i):
        there = (own_p + i) % plane
        return remote(
            partial.at[:, c, there],
            near_return.at[c, own_p],
            n_send.at[2],
            n_recv.at[6],
            own_z * plane + there,
            own_x,
        )

    def near_q_own(c):
        return pltpu.make_async_copy(
            partial.at[:, c, own_p], near_return.at[c, own_p], own_sem.at[2 * groups + 7]
        )

    def answer_copy(i):
        line = (own_y + i) % lines
        return remote(
            attended_back.at[line],
            attended.at[own_y],
            a_send.at[2],
            a_recv.at[2],
            own_z * plane + 2 * line + own_core,
            own_x,
        )

    ask_far = remote(
        queries.at[pl.ds(2, 2)], queries.at[pl.ds(4, 2)], a_send.at[4], a_recv.at[4], mirror, own_x
    )
    answer_far = remote(
        far_part, attended_back.at[pl.ds(2, 2)], a_send.at[5], a_recv.at[5], mirror, own_x
    )
    k_own = pltpu.make_async_copy(
        kv_own.at[own_y], kv_all.at[own_z, own_core, own_y], own_sem.at[2 * groups + 1]
    )
    ask_own = pltpu.make_async_copy(query_own.at[own_y], queries.at[own_y], own_sem.at[2 * groups + 2])
    answer_own = pltpu.make_async_copy(
        attended_back.at[own_y], attended.at[own_y], own_sem.at[2 * groups + 3]
    )

    def mixer_copy(kind, way):
        part = pl.ds(way * mixer_half, mixer_half)
        src, dst = (
            (mixer_part.at[opposite, part], mixer_first.at[way]),
            (mixer_part.at[side[way]], mixer_second.at[way]),
        )[kind]
        return remote(src, dst, s_send.at[4 + kind], s_recv.at[4 + kind], own_ep, side[way])

    first_z = pltpu.make_async_copy(outgoing.at[own_z], stage.at[0], own_sem.at[2 * groups])
    loads = [
        pltpu.make_async_copy(src, dst, weight_sem.at[n])
        for n, (src, dst) in enumerate(
            (
                (shared_gate_hbm, shared_gate_w),
                (shared_up_hbm, shared_up_w),
                (shared_down_hbm, shared_down_w),
                (gate_hbm, gate_w),
                (up_hbm, up_w),
                (down_hbm, down_w),
                (mixer_hbm, mixer_w),
            )
        )
    ]

    barrier = pltpu.get_barrier_semaphore()

    def greet(ep, tp):
        pl.semaphore_signal(
            barrier, inc=1, device_id=(ep, tp), device_id_type=pl.DeviceIdType.MESH
        )

    for k in range(1, groups):
        greet(((own_z + k) % groups) * plane + own_p, own_x)
    for k in range(1, plane):
        greet(own_z * plane + (own_p + k) % plane, own_x)
    greet(own_ep, right)
    greet(own_ep, left)
    for load in loads:
        load.start()

    normed[...] = root_norm(input_ref[...].astype(f32), entry_gain_ref[...]).astype(bf16)

    lane = lax.broadcasted_iota(jnp.int32, (tokens, 128), 1)
    low = lane < head_size
    bias_rows = bias_ref[...].astype(f32)
    tri_row = lax.broadcasted_iota(jnp.int32, tri_ref.shape, 0)
    tri_column = lax.broadcasted_iota(jnp.int32, tri_ref.shape, 1)
    tri_ref[...] = jnp.where(tri_row > tri_column, 1.0, 0.0).astype(bf16)
    for head in range(lines):
        column = (head // 2) * 128

        def placed(ref, upper):
            group = ref[:, column : column + 128].astype(f32)
            return group if head % 2 == upper else pltpu.roll(group, head_size, 1)

        kv_own[head, :tokens] = jnp.where(low, placed(key_ref, 0), placed(value_ref, 1)).astype(bf16)
        kv_own[head, tokens:] = jnp.broadcast_to(bias_rows[head : head + 1], (16, 128)).astype(bf16)
        query_own[head] = jnp.where(low, placed(query_ref, 0) * head_size**-0.5, 0.0).astype(bf16)

    expert_row = lax.broadcasted_iota(jnp.int32, (slots // CAPACITY, shared_rows), 0)
    named = [(expert_row == index_ref[k : k + 1]).astype(f32) for k in range(2)]
    earlier = (
        lax.broadcasted_iota(jnp.int32, (shared_rows, shared_rows), 0)
        < lax.broadcasted_iota(jnp.int32, (shared_rows, shared_rows), 1)
    ).astype(f32).astype(bf16)
    before = jnp.dot((named[0] + named[1]).astype(bf16), earlier, preferred_element_type=f32)
    meta[0] = jnp.zeros((8, 128), f32)
    for k in range(2):
        rank = jnp.sum(named[k] * before, axis=0, keepdims=True)
        meta[0, k : k + 1, :shared_rows] = index_ref[k : k + 1].astype(f32) * CAPACITY + rank
        meta[0, 2 + k : 3 + k, :shared_rows] = weight_ref[k : k + 1]

    def slot_hits(j, first, count):
        number = (lax.broadcasted_iota(jnp.int32, (count, shared_rows), 0) + first).astype(f32)
        return [number == meta[j, k : k + 1, :shared_rows] for k in range(2)]

    def picked(j, first, count):
        hits = slot_hits(j, first, count)
        return (hits[0] | hits[1]).astype(f32).astype(bf16)

    def weighted(j, first, count):
        hits = slot_hits(j, first, count)
        return jnp.where(hits[0], meta[j, 2:3, :shared_rows], 0.0) + jnp.where(
            hits[1], meta[j, 3:4, :shared_rows], 0.0
        )

    def chunk_first(c):
        return ((own_z + offset(c)) % groups) * block_slots

    def halves(value):
        high = value.astype(bf16)
        return high, (value - high.astype(f32)).astype(bf16)

    outgoing[...] = (
        jnp.dot(picked(0, 0, slots), normed[...], preferred_element_type=f32)
        .astype(bf16)
        .reshape(outgoing.shape)
    )
    for c in range(kept, groups):
        part = slice((c - kept) * block_slots, (c - kept + 1) * block_slots)
        mixing_high[part], mixing_low[part] = halves(weighted(0, chunk_first(c), block_slots))
    running[...] = jnp.zeros_like(running)
    carried[...] = jnp.zeros_like(carried)
    first_z.start()
    k_own.start()
    ask_own.start()
    pl.semaphore_wait(barrier, groups + plane)

    for way in range(2):
        shared_copy(0, way).start()
        meta_copy(way).start()
    for c in range(near, min(groups, near + 4)):
        z_copy(c).start()
    for i in range(1, lines):
        k_copy(i).start()
        ask_copy(i).start()
    first_z.wait()

    def compute_shared():
        def one_block(source, target):
            block = source[...]
            gate = jnp.dot(block, shared_gate_w[...], preferred_element_type=f32)
            up = jnp.dot(block, shared_up_w[...], preferred_element_type=f32)
            hidden = silu_product(gate, up)
            target[...] = jnp.dot(hidden, shared_down_w[...], preferred_element_type=f32).astype(bf16)

        one_block(normed, shared_part.at[0])
        for j in range(3):
            one_block(neighbours.at[j], shared_part.at[j + 1])

    def compute_rows(c):
        count = 4 * plane * CAPACITY
        for e in range(experts):
            block = rows[:, c, :, e].reshape(count, width)
            gate = jnp.dot(block, gate_w[e], preferred_element_type=f32)
            up = jnp.dot(block, up_w[e], preferred_element_type=f32)
            hidden = silu_product(gate, up)
            product = jnp.dot(hidden, down_w[e], preferred_element_type=f32).astype(bf16)
            partial[:, c, :, e] = product.reshape(4, plane, CAPACITY, width)

    def flat(value):
        return value.reshape(-1, width).astype(f32)

    def add_first(c):
        for way in range(2):
            part = pl.ds(way * half, half)
            total = flat(partial[2 - way, c, part]) + flat(first_sum[way, c])
            partial[2 - way, c, part] = total.astype(bf16).reshape(half, experts, CAPACITY, width)

    def add_second(c):
        total = flat(partial[0, c]) + flat(second_sum[0, c]) + flat(second_sum[1, c])
        result[c] = total.astype(bf16).reshape(plane, experts, CAPACITY, width)

    def gather_near():
        for j in range(1, 4):
            picks = jnp.concatenate([picked(j, chunk_first(c), block_slots) for c in range(near)], axis=0)
            chosen = jnp.dot(picks, neighbours[j - 1], preferred_element_type=f32).astype(bf16)
            near_out[:, :, j - 1] = chosen.reshape(near, plane, experts, CAPACITY, width)

    def combine_near():
        for j in range(4):
            mixing = weighted(j, chunk_first(0), block_slots)
            found = near_return[0, :, j].reshape(block_slots, width)
            total = shared_part[j].astype(f32)
            for piece in halves(mixing):
                total += lax.dot_general(
                    piece, found, (((0,), (0,)), ((), ())), preferred_element_type=f32
                )
            shared_part[j] = total.astype(bf16)

    first_turns = own_z + 1
    turns = groups + 1
    share = (turns + 2) // 3

    def attend_turn(turn, unused):
        second = jnp.where(turn >= first_turns, 1, 0)
        query_z = own_z + second * (groups - 1 - 2 * own_z)
        key_z = query_z - (turn - second * first_turns)

        def run(masked):
            query = queries[pl.ds(4 * second, 2)].reshape(2 * tokens, 128)
            blocks, biases, masks = [], [], []
            for line in range(lines - 1, -1, -1):
                pair = [kv_all[key_z, core, line] for core in range(2)]
                blocks.append(jnp.concatenate([b[:tokens] for b in pair], axis=0))
                biases.append(
                    jnp.concatenate([b[tokens:][:1] for b in pair], axis=1).astype(f32)
                )
                if masked:
                    row = lax.broadcasted_iota(jnp.int32, (2 * tokens, 2 * tokens), 0)
                    column = lax.broadcasted_iota(jnp.int32, (2 * tokens, 2 * tokens), 1)
                    limit = (2 * second - line) * 2 * tokens + own_core * tokens
                    masks.append(column - (row + (row // tokens) * tokens) < limit)
                else:
                    masks.append(None)
            out, carry = stick_turn(query, blocks, biases, carried[second], tri_ref[...], masks)
            running[second] = running[second] + out
            carried[second] = carry

        @pl.when(key_z == query_z)
        def _():
            run(True)

        @pl.when(key_z != query_z)
        def _():
            run(False)

        return unused

    def finish_attention():
        low2 = lax.broadcasted_iota(jnp.int32, (2 * tokens, 128), 1) < head_size
        even = own_y % 2 == 0
        for second, target in ((0, attended_back.at[pl.ds(0, 2)]), (1, far_part)):
            value = running[second]
            value = jnp.where(even, pltpu.roll(value, head_size, 1), value)
            target[...] = value.astype(bf16).reshape(2, tokens, 128)

    def mix():
        low1 = lax.broadcasted_iota(jnp.int32, (tokens, 128), 1) < head_size
        groups_of_two = [
            jnp.where(low1, attended[2 * n].astype(f32), attended[2 * n + 1].astype(f32)).astype(bf16)
            for n in range(lines // 2)
        ]
        gathered = jnp.concatenate(groups_of_two, axis=1)
        product = jnp.dot(gathered, mixer_w[...], preferred_element_type=f32).astype(bf16)
        mixer_part[...] = product.reshape(4, mixer_rows, width)

    def chunk(i):
        return i + near - (i // max(far, 1)) * summed

    def step(s, unused):
        @pl.when(s < far)
        def _():
            c = s + near
            z_copy(c).wait_recv()
            p_own(c).start()
            for i in range(1, plane):
                p_copy(c, i).start()

        @pl.when(s == 1)
        def _():
            arrived(kv_all.at[own_z, own_core, outer], a_recv.at[0])
            k_own.wait()
            for way in range(2):
                if hops[way] > 0:
                    ring_copy(way, 0).start()
            core_own().start()
            for c in range(near + 4, groups):
                z_copy(c).start()
            arrived(queries.at[outer], a_recv.at[1])
            ask_own.wait()
            ask_far.start()

        @pl.when(s == 2)
        def _():
            shared_arrived(0)
            arrived(meta.at[pl.ds(1, 2)], m_recv.at[0])
            for way in range(2):
                shared_copy(1, way).start()
            meta_far.start()

        @pl.when((s >= 1) & (s < far + 1))
        def _():
            c = s - 1 + near
            p_arrived(c)
            for way in range(2):
                x_copy(c, way).start()

        @pl.when((s >= 2) & (s < far + 2))
        def _():
            c = s - 2 + near
            x_arrived(0, c)
            for way in range(2):
                f_copy(c, way).start()

        for r in range(hops[1]):

            @pl.when(s == RING_STEPS[r])
            def _():
                for way in range(2):
                    if r < hops[way]:
                        ring_copy(way, r).wait_recv()
                        if r + 1 < hops[way]:
                            ring_copy(way, r + 1).start()
                        core_copy(way, r).start()

        @pl.when(s == 3)
        def _():
            shared_arrived(1)
            meta_far.wait_recv()
            gather_near()
            for c in range(1, near):
                near_z(c).start()
                z_copy(c).start()
            p_own(0).start()
            near_p_own(0).start()
            for i in range(1, plane):
                p_copy(0, i).start()
                near_p(0, i).start()

        @pl.when(s == 4)
        def _():
            for load in loads:
                load.wait()

        @pl.when((s >= 4) & (s < far + 4))
        def _():
            c = s - 4 + near
            x_arrived(1, c)
            compute_rows(c)
            for way in range(2):
                r_copy(c, way).start()

        @pl.when(s == 6)
        def _():
            p_arrived(0)
            near_arrived(0)
            compute_rows(0)
            near_q_own(0).start()
            for i in range(1, plane):
                near_q(0, i).start()

        for c in range(1, near):

            @pl.when(s == far + 3 + c)
            def _():
                p_arrived(c)
                near_arrived(c)
                compute_rows(c)
                for way in range(2):
                    r_copy(c, way).start()

        @pl.when((s >= 5) & (s < summed + 5))
        def _():
            c = chunk(s - 5)
            x_arrived(2, c)
            add_first(c)
            for way in range(2):
                t_copy(c, way).start()

        @pl.when((s >= 6) & (s < summed + 6))
        def _():
            c = chunk(s - 6)
            x_arrived(3, c)
            add_second(c)
            q_own(c).start()
            for i in range(1, plane):
                q_copy(c, i).start()

        @pl.when((s >= 8) & (s < summed + 8))
        def _():
            c = chunk(s - 8)
            q_arrived(c)
            b_copy(c).start()

        @pl.when(s == 5)
        def _():
            compute_shared()

        if near > 1:

            @pl.when(s == 7)
            def _():
                for c in range(1, near):
                    near_z(c).wait_recv()
                    z_copy(c).wait_recv()
                    p_own(c).start()
                    near_p_own(c).start()
                    for i in range(1, plane):
                        p_copy(c, i).start()
                        near_p(c, i).start()

        @pl.when(s == 8)
        def _():
            arrived(kv_all.at[:, 0], a_recv.at[3])
            ask_far.wait_recv()

        @pl.when((s >= 8) & (s < 11))
        def _():
            first = (s - 8) * share
            lax.fori_loop(first, jnp.minimum(first + share, turns), attend_turn, 0)

        @pl.when(s == 10)
        def _():
            finish_attention()
            answer_far.start()

        @pl.when(s == 10)
        def _():
            arrived(near_return.at[0, others], n_recv.at[6])
            near_q_own(0).wait()
            combine_near()
            for way in range(2):
                shared_copy(2, way).start()

        @pl.when(s == 11)
        def _():
            shared_arrived(2)
            for way in range(2):
                part = pl.ds(way * shared_half, shared_half)
                shared_part[2 - way, part] = (
                    shared_part[2 - way, part].astype(f32) + shared_first[way].astype(f32)
                ).astype(bf16)
                shared_copy(3, way).start()

        @pl.when(s == 12)
        def _():
            answer_far.wait_recv()
            answer_own.start()
            for i in range(1, lines):
                answer_copy(i).start()

        @pl.when(s == 13)
        def _():
            arrived(attended.at[outer], a_recv.at[2])
            answer_own.wait()
            mix()
            for way in range(2):
                mixer_copy(0, way).start()

        return unused

    lax.fori_loop(0, max(summed + 8, 14), step, 0)

    shared_arrived(4)
    for way in range(2):
        part = pl.ds(way * mixer_half, mixer_half)
        mixer_part[side[way], part] = (
            mixer_part[side[way], part].astype(f32) + mixer_first[way].astype(f32)
        ).astype(bf16)
        mixer_copy(1, way).start()
    arrived(back, b_recv.at[0])
    rows_back = back[...].reshape(summed * block_slots, width)
    combined = sum(
        lax.dot_general(m[...], rows_back, (((0,), (0,)), ((), ())), preferred_element_type=f32)
        for m in (mixing_high, mixing_low)
    )
    shared_arrived(3)
    combined = (
        combined
        + shared_part[0].astype(f32)
        + shared_second[0].astype(f32)
        + shared_second[1].astype(f32)
    )
    expert_out[...] = root_norm(combined, exit_gain_ref[...]).astype(bf16)

    shared_arrived(5)
    mixer_out[...] = root_norm(
        mixer_part[own_x].astype(f32) + mixer_second[0].astype(f32) + mixer_second[1].astype(f32),
        mixer_gain_ref[...],
    ).astype(bf16)
    for ref, sem in (
        (stage.at[pl.ds(0, groups - 1)], z_send.at[0]),
        (stage.at[:, others], p_send.at[0]),
        (rows.at[pl.ds(0, 2), pl.ds(0, far)], x_send.at[0]),
        (rows.at[0, pl.ds(0, far)], x_send.at[1]),
        (partial.at[0, pl.ds(0, summed)], x_send.at[2]),
        (partial.at[pl.ds(0, 2), pl.ds(0, summed)], x_send.at[3]),
        (returned.at[pl.ds(0, summed), others], q_send.at[0]),
        (returned.at[pl.ds(0, summed)], b_send.at[0]),
        (meta.at[pl.ds(1, 3)], m_send.at[0]),
        (kv_all.at[own_z, own_core, outer], a_send.at[0]),
        (queries.at[outer], a_send.at[1]),
        (attended.at[outer], a_send.at[2]),
        (kv_all.at[:, 0], a_send.at[3]),
        (kv_all.at[pl.ds(0, groups - 1), 0], a_send.at[6]),
        (near_out.at[:, others], n_send.at[1]),
        (near_return.at[0, others], n_send.at[2]),
    ):
        left_here(ref, sem)
    if near > 1:
        left_here(near_stage.at[pl.ds(0, near - 1)], n_send.at[0])
    for kind, ref in enumerate(shared_landing):
        left_here(ref, s_send.at[kind])
    ask_far.wait_send()
    answer_far.wait_send()


def on_device(
    query_rows,
    key_rows,
    value_rows,
    key_bias,
    mixer_weight,
    mixer_gain,
    routed_input,
    entry_gain,
    expert_index,
    route_weights,
    expert_gate,
    expert_up,
    expert_down,
    shared_gate,
    shared_up,
    shared_down,
    exit_gain,
):
    bf16, f32 = jnp.bfloat16, jnp.float32
    plane = PLANE
    groups = lax.axis_size("ep") // plane
    lines, half = plane // 2, plane // 2
    tokens = query_rows.shape[0]
    count, width = routed_input.shape
    experts = expert_gate.shape[0]
    block = (plane, experts, CAPACITY, width)
    near = min(NEAR, groups)
    kept_slots = (groups - 1) * plane * experts * CAPACITY
    vmem = pl.BlockSpec(memory_space=pltpu.VMEM)
    hbm = pl.BlockSpec(memory_space=pl.ANY)
    weights = (expert_gate, expert_up, expert_down, shared_gate, shared_up, shared_down)
    dma = pltpu.SemaphoreType.DMA
    return pl.pallas_call(
        functools.partial(program_kernel, groups, plane),
        out_shape=(
            jax.ShapeDtypeStruct((tokens // 4, width), bf16),
            jax.ShapeDtypeStruct((count, width), bf16),
        ),
        in_specs=[vmem] * 4 + [hbm] + [vmem] * 6 + [hbm] * 6,
        out_specs=(vmem, vmem),
        scratch_shapes=[
            pltpu.VMEM((count, width), bf16),
            pltpu.VMEM((groups,) + block, bf16),
            pltpu.VMEM((groups - 1,) + block, bf16),
            pltpu.VMEM((groups,) + block, bf16),
            pltpu.VMEM((4, groups) + block, bf16),
            pltpu.VMEM((4, groups) + block, bf16),
            pltpu.VMEM((2, groups, half) + block[1:], bf16),
            pltpu.VMEM((2, groups) + block, bf16),
            pltpu.VMEM((groups,) + block, bf16),
            pltpu.VMEM((groups,) + block, bf16),
            pltpu.VMEM((3, count, width), bf16),
            pltpu.VMEM((4, count, width), bf16),
            pltpu.VMEM((2, count // 2, width), bf16),
            pltpu.VMEM((2, count, width), bf16),
            pltpu.VMEM((lines, tokens + 16, 128), bf16),
            pltpu.VMEM((lines, tokens, 128), bf16),
            pltpu.VMEM((groups, 2, lines, tokens + 16, 128), bf16),
            pltpu.VMEM((6, tokens, 128), bf16),
            pltpu.VMEM((2, 2 * tokens, 128), f32),
            pltpu.VMEM((2, 2 * tokens, 128), f32),
            pltpu.VMEM((2, tokens, 128), bf16),
            pltpu.VMEM((lines, tokens, 128), bf16),
            pltpu.VMEM((lines, tokens, 128), bf16),
            pltpu.VMEM((4, tokens // 4, width), bf16),
            pltpu.VMEM((2, tokens // 8, width), bf16),
            pltpu.VMEM((2, tokens // 4, width), bf16),
            pltpu.VMEM(mixer_weight.shape, bf16),
        ]
        + [pltpu.VMEM(w.shape, bf16) for w in weights]
        + [
            pltpu.VMEM((kept_slots, count), bf16),
            pltpu.VMEM((kept_slots, count), bf16),
            pltpu.VMEM((2 * tokens, 2 * tokens), bf16),
            pltpu.VMEM((4, 8, 128), f32),
            pltpu.VMEM((near, plane, 3) + block[1:], bf16),
            pltpu.VMEM((max(near - 1, 1), plane, 3) + block[1:], bf16),
            pltpu.VMEM((1, plane, 4) + block[1:], bf16),
            dma((7,)),
            dma((2 * groups + 8,)),
            dma((1,)),
            dma((groups,)),
            dma((1,)),
            dma((groups,)),
            dma((4,)),
            dma((4, groups)),
            dma((1,)),
            dma((groups,)),
            dma((1,)),
            dma((1,)),
            dma((6,)),
            dma((6,)),
            dma((7,)),
            dma((6 + groups,)),
            dma((3,)),
            dma((7,)),
            dma((1,)),
            dma((2,)),
        ],
        compiler_params=pltpu.CompilerParams(
            collective_id=1, has_side_effects=True, vmem_limit_bytes=62 << 20
        ),
        name="program",
    )(
        query_rows,
        key_rows,
        value_rows,
        jnp.transpose(key_bias),
        mixer_weight,
        mixer_gain.reshape(1, width),
        routed_input,
        entry_gain.reshape(1, width),
        jnp.transpose(expert_index),
        jnp.transpose(route_weights),
        exit_gain.reshape(1, width),
        *weights,
    )


def solution(mesh):
    in_specs = (
        P("ep", "tp"),
        P("ep", "tp"),
        P("ep", "tp"),
        P("ep", "tp"),
        P("tp", None),
        P(),
        P(("ep", "tp"), None),
        P(),
        P(("ep", "tp"), None),
        P(("ep", "tp"), None),
        P("ep", None, "tp"),
        P("ep", None, "tp"),
        P("ep", "tp", None),
        P(None, "tp"),
        P(None, "tp"),
        P("tp", None),
        P(),
    )
    out_specs = (P(("ep", "tp"), None), P(("ep", "tp"), None))
    return jax.shard_map(
        on_device, mesh=mesh, in_specs=in_specs, out_specs=out_specs, check_vma=False
    )
```

```python
import functools

import jax
import jax.numpy as jnp
from jax import lax
from jax.experimental import pallas as pl
from jax.experimental.pallas import tpu as pltpu
from jax.sharding import PartitionSpec as P

EPS = 1e-06
PLANE = 8
CAPACITY = 2
NEAR = 2
RING_STEPS = (3, 5, 6, 7)


def root_norm(values, gain_row):
    return values * lax.rsqrt(jnp.mean(values * values, axis=-1, keepdims=True) + EPS) * gain_row


def stick_turn(query, blocks, biases, carry, tri, masks):
    keys = tri.shape[0]
    levels, weights = [], []
    for block, bias, mask in zip(blocks, biases, masks):
        score = (
            lax.dot_general(
                query, block, (((1,), (1,)), ((), ())), preferred_element_type=jnp.float32
            )
            + bias
        )
        fail = jnp.maximum(score, 0.0) + jnp.log(1.0 + jnp.exp(-jnp.abs(score)))
        counted = fail if mask is None else jnp.where(mask, fail, 0.0)
        sums = jnp.dot(counted.astype(jnp.bfloat16), tri, preferred_element_type=jnp.float32)
        total = jnp.broadcast_to(sums[:, 0:1] + counted[:, 0:1], carry.shape)
        levels.append(((score - fail) - sums, total))
    for (level, total), mask in zip(levels, masks):
        weight = jnp.exp(level - jnp.concatenate([carry] * (keys // carry.shape[1]), axis=1))
        if mask is not None:
            weight = jnp.where(mask, weight, 0.0)
        weights.append(weight.astype(jnp.bfloat16))
        carry = carry + total
    out = jnp.dot(
        jnp.concatenate(weights, axis=1),
        jnp.concatenate(blocks, axis=0),
        preferred_element_type=jnp.float32,
    )
    return out, carry


def silu_product(gate, up):
    return (gate / (1.0 + jnp.exp(-gate)) * up).astype(jnp.bfloat16)


def program_kernel(
    groups,
    plane,
    query_ref,
    key_ref,
    value_ref,
    bias_ref,
    mixer_hbm,
    mixer_gain_ref,
    input_ref,
    entry_gain_ref,
    index_ref,
    weight_ref,
    exit_gain_ref,
    gate_hbm,
    up_hbm,
    down_hbm,
    shared_gate_hbm,
    shared_up_hbm,
    shared_down_hbm,
    mixer_out,
    expert_out,
    normed,
    outgoing,
    back,
    stage,
    rows,
    partial,
    first_sum,
    second_sum,
    result,
    returned,
    neighbours,
    shared_part,
    shared_first,
    shared_second,
    kv_own,
    query_own,
    kv_all,
    queries,
    running,
    carried,
    far_part,
    attended_back,
    attended,
    mixer_part,
    mixer_first,
    mixer_second,
    mixer_w,
    gate_w,
    up_w,
    down_w,
    shared_gate_w,
    shared_up_w,
    shared_down_w,
    mixing_high,
    mixing_low,
    tri_ref,
    meta,
    near_out,
    near_stage,
    near_return,
    weight_sem,
    own_sem,
    z_send,
    z_recv,
    p_send,
    p_recv,
    x_send,
    x_recv,
    q_send,
    q_recv,
    b_send,
    b_recv,
    s_send,
    s_recv,
    a_send,
    a_recv,
    n_send,
    n_recv,
    m_send,
    m_recv,
):
    f32, bf16 = jnp.float32, jnp.bfloat16
    own_ep = lax.axis_index("ep")
    own_x = lax.axis_index("tp")
    own_z = own_ep // plane
    own_p = own_ep % plane
    own_y = own_p // 2
    own_core = own_p % 2
    lines = plane // 2
    half = plane // 2
    right = (own_x + 1) % 4
    left = (own_x + 3) % 4
    opposite = (own_x + 2) % 4
    side = (right, left)
    experts, width = gate_w.shape[0], gate_w.shape[1]
    shared_rows = normed.shape[0]
    shared_half = shared_rows // 2
    tokens = key_ref.shape[0]
    head_size = query_ref.shape[1] // lines
    mixer_rows = tokens // 4
    mixer_half = mixer_rows // 2
    block_slots = plane * experts * CAPACITY
    slots = groups * block_slots
    near = min(NEAR, groups)
    far = groups - near
    kept = 1
    summed = groups - kept

    def remote(src, dst, send_sem, recv_sem, ep, tp):
        return pltpu.make_async_remote_copy(
            src_ref=src,
            dst_ref=dst,
            send_sem=send_sem,
            recv_sem=recv_sem,
            device_id=(ep, tp),
            device_id_type=pl.DeviceIdType.MESH,
        )

    def offset(c):
        odd = c % 2
        return (odd * (groups - (c + 1) // 2) + (1 - odd) * (c // 2)) % groups

    def z_copy(c):
        there = (own_z + offset(c)) % groups
        return remote(
            outgoing.at[there], stage.at[c], z_send.at[0], z_recv.at[c], there * plane + own_p, own_x
        )

    def p_copy(c, i):
        there = (own_p + i) % plane
        return remote(
            stage.at[c, there],
            rows.at[0, c, own_p],
            p_send.at[0],
            p_recv.at[c],
            own_z * plane + there,
            own_x,
        )

    def p_own(c):
        return pltpu.make_async_copy(stage.at[c, own_p], rows.at[0, c, own_p], own_sem.at[c])

    def x_copy(c, way):
        return remote(
            rows.at[0, c], rows.at[1 + way, c], x_send.at[0], x_recv.at[0, c], own_ep, side[way]
        )

    def f_copy(c, way):
        part = pl.ds(way * half, half)
        return remote(
            rows.at[1 + way, c, part],
            rows.at[3, c, part],
            x_send.at[1],
            x_recv.at[1, c],
            own_ep,
            side[way],
        )

    def r_copy(c, way):
        return remote(
            partial.at[3, c, pl.ds(way * half, half)],
            first_sum.at[way, c],
            x_send.at[2],
            x_recv.at[2, c],
            own_ep,
            side[way],
        )

    def t_copy(c, way):
        return remote(
            partial.at[2 - way, c],
            second_sum.at[way, c],
            x_send.at[3],
            x_recv.at[3, c],
            own_ep,
            side[way],
        )

    def q_copy(c, i):
        there = (own_p + i) % plane
        return remote(
            result.at[c, there],
            returned.at[c, own_p],
            q_send.at[0],
            q_recv.at[c],
            own_z * plane + there,
            own_x,
        )

    def q_own(c):
        return pltpu.make_async_copy(result.at[c, own_p], returned.at[c, own_p], own_sem.at[groups + c])

    def b_copy(c):
        there = (own_z + groups - offset(c)) % groups
        return remote(
            returned.at[c], back.at[c - kept], b_send.at[0], b_recv.at[0], there * plane + own_p, own_x
        )

    def shared_copy(kind, way):
        part = pl.ds(way * shared_half, shared_half)
        src, dst = (
            (normed, neighbours.at[way]),
            (neighbours.at[way, part], neighbours.at[2, part]),
            (shared_part.at[3, part], shared_first.at[way]),
            (shared_part.at[2 - way], shared_second.at[way]),
        )[kind]
        return remote(src, dst, s_send.at[kind], s_recv.at[kind], own_ep, side[way])

    mirror = (groups - 1 - own_z) * plane + own_p
    partner = own_z * plane + own_p + 1 - 2 * own_core

    def k_copy(i):
        line = (own_y + i) % lines
        return remote(
            kv_own.at[line],
            kv_all.at[own_z, own_core, own_y],
            a_send.at[0],
            a_recv.at[0],
            own_z * plane + 2 * line + own_core,
            own_x,
        )

    def ask_copy(i):
        line = (own_y + i) % lines
        return remote(
            query_own.at[line],
            queries.at[own_y],
            a_send.at[1],
            a_recv.at[1],
            own_z * plane + 2 * line + own_core,
            own_x,
        )

    def ring_copy(way, r):
        source = (own_z + groups + (2 * way - 1) * r) % groups
        there = (own_z + groups + 1 - 2 * way) % groups
        block = kv_all.at[source, own_core]
        return remote(
            block, block, a_send.at[6], a_recv.at[6 + way * hops[0] + r], there * plane + own_p, own_x
        )

    def core_copy(way, r):
        source = (own_z + groups + (2 * way - 1) * (r + 1)) % groups
        block = kv_all.at[source, own_core]
        return remote(block, block, a_send.at[3], a_recv.at[3], partner, own_x)

    def core_own():
        block = kv_all.at[own_z, own_core]
        return remote(block, block, a_send.at[3], a_recv.at[3], partner, own_x)

    hops = ((groups - 1) // 2, groups // 2)
    others = pl.ds(0, plane - 1)
    outer = pl.ds(0, lines - 1)

    def meter(ref, send_sem, recv_sem):
        return remote(ref, ref, send_sem, recv_sem, own_ep, right)

    def arrived(ref, sem):
        meter(ref, sem, sem).wait_recv()

    def left_here(ref, sem):
        meter(ref, sem, sem).wait_send()

    shared_landing = (
        neighbours.at[pl.ds(0, 2)],
        neighbours.at[2],
        shared_first,
        shared_second,
        mixer_first,
        mixer_second,
    )

    def shared_arrived(kind):
        arrived(shared_landing[kind], s_recv.at[kind])

    def x_arrived(kind, c):
        landing = (
            rows.at[pl.ds(1, 2), c],
            rows.at[3, c],
            first_sum.at[:, c],
            second_sum.at[:, c],
        )[kind]
        arrived(landing, x_recv.at[kind, c])

    def p_arrived(c):
        arrived(rows.at[0, c, others], p_recv.at[c])
        p_own(c).wait()

    def near_arrived(c):
        arrived(rows.at[pl.ds(1, 3), c, others], n_recv.at[3 + c])
        near_p_own(c).wait()

    def q_arrived(c):
        arrived(returned.at[c, others], q_recv.at[c])
        q_own(c).wait()


    def meta_copy(way):
        return remote(
            meta.at[0], meta.at[1 + way], m_send.at[0], m_recv.at[0], own_ep, side[way]
        )

    meta_far = remote(meta.at[1], meta.at[3], m_send.at[0], m_recv.at[1], own_ep, right)

    def near_z(c):
        there = (own_z + offset(c)) % groups
        return remote(
            near_out.at[c],
            near_stage.at[c - 1],
            n_send.at[0],
            n_recv.at[c],
            there * plane + own_p,
            own_x,
        )

    def near_source(c, place):
        return near_out.at[0, place] if c == 0 else near_stage.at[c - 1, place]

    def near_p(c, i):
        there = (own_p + i) % plane
        return remote(
            near_source(c, there),
            rows.at[pl.ds(1, 3), c, own_p],
            n_send.at[1],
            n_recv.at[3 + c],
            own_z * plane + there,
            own_x,
        )

    def near_p_own(c):
        return pltpu.make_async_copy(
            near_source(c, own_p), rows.at[pl.ds(1, 3), c, own_p], own_sem.at[2 * groups + 4 + c]
        )

    def near_q(c, i):
        there = (own_p + i) % plane
        return remote(
            partial.at[:, c, there],
            near_return.at[c, own_p],
            n_send.at[2],
            n_recv.at[6],
            own_z * plane + there,
            own_x,
        )

    def near_q_own(c):
        return pltpu.make_async_copy(
            partial.at[:, c, own_p], near_return.at[c, own_p], own_sem.at[2 * groups + 7]
        )

    def answer_copy(i):
        line = (own_y + i) % lines
        return remote(
            attended_back.at[line],
            attended.at[own_y],
            a_send.at[2],
            a_recv.at[2],
            own_z * plane + 2 * line + own_core,
            own_x,
        )

    ask_far = remote(
        queries.at[pl.ds(2, 2)], queries.at[pl.ds(4, 2)], a_send.at[4], a_recv.at[4], mirror, own_x
    )
    answer_far = remote(
        far_part, attended_back.at[pl.ds(2, 2)], a_send.at[5], a_recv.at[5], mirror, own_x
    )
    k_own = pltpu.make_async_copy(
        kv_own.at[own_y], kv_all.at[own_z, own_core, own_y], own_sem.at[2 * groups + 1]
    )
    ask_own = pltpu.make_async_copy(query_own.at[own_y], queries.at[own_y], own_sem.at[2 * groups + 2])
    answer_own = pltpu.make_async_copy(
        attended_back.at[own_y], attended.at[own_y], own_sem.at[2 * groups + 3]
    )

    def mixer_copy(kind, way):
        part = pl.ds(way * mixer_half, mixer_half)
        src, dst = (
            (mixer_part.at[opposite, part], mixer_first.at[way]),
            (mixer_part.at[side[way]], mixer_second.at[way]),
        )[kind]
        return remote(src, dst, s_send.at[4 + kind], s_recv.at[4 + kind], own_ep, side[way])

    first_z = pltpu.make_async_copy(outgoing.at[own_z], stage.at[0], own_sem.at[2 * groups])
    loads = [
        pltpu.make_async_copy(src, dst, weight_sem.at[n])
        for n, (src, dst) in enumerate(
            (
                (shared_gate_hbm, shared_gate_w),
                (shared_up_hbm, shared_up_w),
                (shared_down_hbm, shared_down_w),
                (gate_hbm, gate_w),
                (up_hbm, up_w),
                (down_hbm, down_w),
                (mixer_hbm, mixer_w),
            )
        )
    ]

    barrier = pltpu.get_barrier_semaphore()

    def greet(ep, tp):
        pl.semaphore_signal(
            barrier, inc=1, device_id=(ep, tp), device_id_type=pl.DeviceIdType.MESH
        )

    for k in range(1, groups):
        greet(((own_z + k) % groups) * plane + own_p, own_x)
    for k in range(1, plane):
        greet(own_z * plane + (own_p + k) % plane, own_x)
    greet(own_ep, right)
    greet(own_ep, left)
    for load in loads:
        load.start()

    normed[...] = root_norm(input_ref[...].astype(f32), entry_gain_ref[...]).astype(bf16)

    lane = lax.broadcasted_iota(jnp.int32, (tokens, 128), 1)
    low = lane < head_size
    bias_rows = bias_ref[...].astype(f32)
    tri_row = lax.broadcasted_iota(jnp.int32, tri_ref.shape, 0)
    tri_column = lax.broadcasted_iota(jnp.int32, tri_ref.shape, 1)
    tri_ref[...] = jnp.where(tri_row > tri_column, 1.0, 0.0).astype(bf16)
    for head in range(lines):
        column = (head // 2) * 128

        def placed(ref, upper):
            group = ref[:, column : column + 128].astype(f32)
            return group if head % 2 == upper else pltpu.roll(group, head_size, 1)

        kv_own[head, :tokens] = jnp.where(low, placed(key_ref, 0), placed(value_ref, 1)).astype(bf16)
        kv_own[head, tokens:] = jnp.broadcast_to(bias_rows[head : head + 1], (16, 128)).astype(bf16)
        query_own[head] = jnp.where(low, placed(query_ref, 0) * head_size**-0.5, 0.0).astype(bf16)

    expert_row = lax.broadcasted_iota(jnp.int32, (slots // CAPACITY, shared_rows), 0)
    named = [(expert_row == index_ref[k : k + 1]).astype(f32) for k in range(2)]
    earlier = (
        lax.broadcasted_iota(jnp.int32, (shared_rows, shared_rows), 0)
        < lax.broadcasted_iota(jnp.int32, (shared_rows, shared_rows), 1)
    ).astype(f32).astype(bf16)
    before = jnp.dot((named[0] + named[1]).astype(bf16), earlier, preferred_element_type=f32)
    meta[0] = jnp.zeros((8, 128), f32)
    for k in range(2):
        rank = jnp.sum(named[k] * before, axis=0, keepdims=True)
        meta[0, k : k + 1, :shared_rows] = index_ref[k : k + 1].astype(f32) * CAPACITY + rank
        meta[0, 2 + k : 3 + k, :shared_rows] = weight_ref[k : k + 1]

    def slot_hits(j, first, count):
        number = (lax.broadcasted_iota(jnp.int32, (count, shared_rows), 0) + first).astype(f32)
        return [number == meta[j, k : k + 1, :shared_rows] for k in range(2)]

    def picked(j, first, count):
        hits = slot_hits(j, first, count)
        return (hits[0] | hits[1]).astype(f32).astype(bf16)

    def weighted(j, first, count):
        hits = slot_hits(j, first, count)
        return jnp.where(hits[0], meta[j, 2:3, :shared_rows], 0.0) + jnp.where(
            hits[1], meta[j, 3:4, :shared_rows], 0.0
        )

    def chunk_first(c):
        return ((own_z + offset(c)) % groups) * block_slots

    def halves(value):
        high = value.astype(bf16)
        return high, (value - high.astype(f32)).astype(bf16)

    outgoing[...] = (
        jnp.dot(picked(0, 0, slots), normed[...], preferred_element_type=f32)
        .astype(bf16)
        .reshape(outgoing.shape)
    )
    for c in range(kept, groups):
        part = slice((c - kept) * block_slots, (c - kept + 1) * block_slots)
        mixing_high[part], mixing_low[part] = halves(weighted(0, chunk_first(c), block_slots))
    running[...] = jnp.zeros_like(running)
    carried[...] = jnp.zeros_like(carried)
    first_z.start()
    k_own.start()
    ask_own.start()
    pl.semaphore_wait(barrier, groups + plane)

    for way in range(2):
        shared_copy(0, way).start()
        meta_copy(way).start()
    for c in range(near, min(groups, near + 4)):
        z_copy(c).start()
    for i in range(1, lines):
        k_copy(i).start()
        ask_copy(i).start()
    first_z.wait()

    def compute_shared():
        def one_block(source, target):
            block = source[...]
            gate = jnp.dot(block, shared_gate_w[...], preferred_element_type=f32)
            up = jnp.dot(block, shared_up_w[...], preferred_element_type=f32)
            hidden = silu_product(gate, up)
            target[...] = jnp.dot(hidden, shared_down_w[...], preferred_element_type=f32).astype(bf16)

        one_block(normed, shared_part.at[0])
        for j in range(3):
            one_block(neighbours.at[j], shared_part.at[j + 1])

    def compute_rows(c):
        count = 4 * plane * CAPACITY
        for e in range(experts):
            block = rows[:, c, :, e].reshape(count, width)
            gate = jnp.dot(block, gate_w[e], preferred_element_type=f32)
            up = jnp.dot(block, up_w[e], preferred_element_type=f32)
            hidden = silu_product(gate, up)
            product = jnp.dot(hidden, down_w[e], preferred_element_type=f32).astype(bf16)
            partial[:, c, :, e] = product.reshape(4, plane, CAPACITY, width)

    def flat(value):
        return value.reshape(-1, width).astype(f32)

    def add_first(c):
        for way in range(2):
            part = pl.ds(way * half, half)
            total = flat(partial[2 - way, c, part]) + flat(first_sum[way, c])
            partial[2 - way, c, part] = total.astype(bf16).reshape(half, experts, CAPACITY, width)

    def add_second(c):
        total = flat(partial[0, c]) + flat(second_sum[0, c]) + flat(second_sum[1, c])
        result[c] = total.astype(bf16).reshape(plane, experts, CAPACITY, width)

    def gather_near():
        for j in range(1, 4):
            picks = jnp.concatenate([picked(j, chunk_first(c), block_slots) for c in range(near)], axis=0)
            chosen = jnp.dot(picks, neighbours[j - 1], preferred_element_type=f32).astype(bf16)
            near_out[:, :, j - 1] = chosen.reshape(near, plane, experts, CAPACITY, width)

    def combine_near():
        for j in range(4):
            mixing = weighted(j, chunk_first(0), block_slots)
            found = near_return[0, :, j].reshape(block_slots, width)
            total = shared_part[j].astype(f32)
            for piece in halves(mixing):
                total += lax.dot_general(
                    piece, found, (((0,), (0,)), ((), ())), preferred_element_type=f32
                )
            shared_part[j] = total.astype(bf16)

    first_turns = own_z + 1
    turns = groups + 1
    share = (turns + 2) // 3

    def attend_turn(turn, unused):
        second = jnp.where(turn >= first_turns, 1, 0)
        query_z = own_z + second * (groups - 1 - 2 * own_z)
        key_z = query_z - (turn - second * first_turns)

        def run(masked):
            query = queries[pl.ds(4 * second, 2)].reshape(2 * tokens, 128)
            blocks, biases, masks = [], [], []
            for line in range(lines - 1, -1, -1):
                pair = [kv_all[key_z, core, line] for core in range(2)]
                blocks.append(jnp.concatenate([b[:tokens] for b in pair], axis=0))
                biases.append(
                    jnp.concatenate([b[tokens:][:1] for b in pair], axis=1).astype(f32)
                )
                if masked:
                    row = lax.broadcasted_iota(jnp.int32, (2 * tokens, 2 * tokens), 0)
                    column = lax.broadcasted_iota(jnp.int32, (2 * tokens, 2 * tokens), 1)
                    limit = (2 * second - line) * 2 * tokens + own_core * tokens
                    masks.append(column - (row + (row // tokens) * tokens) < limit)
                else:
                    masks.append(None)
            out, carry = stick_turn(query, blocks, biases, carried[second], tri_ref[...], masks)
            running[second] = running[second] + out
            carried[second] = carry

        @pl.when(key_z == query_z)
        def _():
            run(True)

        @pl.when(key_z != query_z)
        def _():
            run(False)

        return unused

    def finish_attention():
        low2 = lax.broadcasted_iota(jnp.int32, (2 * tokens, 128), 1) < head_size
        even = own_y % 2 == 0
        for second, target in ((0, attended_back.at[pl.ds(0, 2)]), (1, far_part)):
            value = running[second]
            value = jnp.where(even, pltpu.roll(value, head_size, 1), value)
            target[...] = value.astype(bf16).reshape(2, tokens, 128)

    def mix():
        low1 = lax.broadcasted_iota(jnp.int32, (tokens, 128), 1) < head_size
        groups_of_two = [
            jnp.where(low1, attended[2 * n].astype(f32), attended[2 * n + 1].astype(f32)).astype(bf16)
            for n in range(lines // 2)
        ]
        gathered = jnp.concatenate(groups_of_two, axis=1)
        product = jnp.dot(gathered, mixer_w[...], preferred_element_type=f32).astype(bf16)
        mixer_part[...] = product.reshape(4, mixer_rows, width)

    def chunk(i):
        return i + near - (i // max(far, 1)) * summed

    def step(s, unused):
        @pl.when(s < far)
        def _():
            c = s + near
            z_copy(c).wait_recv()
            p_own(c).start()
            for i in range(1, plane):
                p_copy(c, i).start()

        @pl.when(s == 1)
        def _():
            arrived(kv_all.at[own_z, own_core, outer], a_recv.at[0])
            k_own.wait()
            for way in range(2):
                if hops[way] > 0:
                    ring_copy(way, 0).start()
            core_own().start()
            for c in range(near + 4, groups):
                z_copy(c).start()
            arrived(queries.at[outer], a_recv.at[1])
            ask_own.wait()
            ask_far.start()

        @pl.when(s == 2)
        def _():
            shared_arrived(0)
            arrived(meta.at[pl.ds(1, 2)], m_recv.at[0])
            for way in range(2):
                shared_copy(1, way).start()
            meta_far.start()

        @pl.when((s >= 1) & (s < far + 1))
        def _():
            c = s - 1 + near
            p_arrived(c)
            for way in range(2):
                x_copy(c, way).start()

        @pl.when((s >= 2) & (s < far + 2))
        def _():
            c = s - 2 + near
            x_arrived(0, c)
            for way in range(2):
                f_copy(c, way).start()

        for r in range(hops[1]):

            @pl.when(s == RING_STEPS[r])
            def _():
                for way in range(2):
                    if r < hops[way]:
                        ring_copy(way, r).wait_recv()
                        if r + 1 < hops[way]:
                            ring_copy(way, r + 1).start()
                        core_copy(way, r).start()

        @pl.when(s == 3)
        def _():
            shared_arrived(1)
            meta_far.wait_recv()
            gather_near()
            for c in range(1, near):
                near_z(c).start()
                z_copy(c).start()
            p_own(0).start()
            near_p_own(0).start()
            for i in range(1, plane):
                p_copy(0, i).start()
                near_p(0, i).start()

        @pl.when(s == 4)
        def _():
            for load in loads:
                load.wait()

        @pl.when((s >= 4) & (s < far + 4))
        def _():
            c = s - 4 + near
            x_arrived(1, c)
            compute_rows(c)
            for way in range(2):
                r_copy(c, way).start()

        @pl.when(s == 6)
        def _():
            p_arrived(0)
            near_arrived(0)
            compute_rows(0)
            near_q_own(0).start()
            for i in range(1, plane):
                near_q(0, i).start()

        for c in range(1, near):

            @pl.when(s == far + 3 + c)
            def _():
                p_arrived(c)
                near_arrived(c)
                compute_rows(c)
                for way in range(2):
                    r_copy(c, way).start()

        @pl.when((s >= 5) & (s < summed + 5))
        def _():
            c = chunk(s - 5)
            x_arrived(2, c)
            add_first(c)
            for way in range(2):
                t_copy(c, way).start()

        @pl.when((s >= 6) & (s < summed + 6))
        def _():
            c = chunk(s - 6)
            x_arrived(3, c)
            add_second(c)
            q_own(c).start()
            for i in range(1, plane):
                q_copy(c, i).start()

        @pl.when((s >= 8) & (s < summed + 8))
        def _():
            c = chunk(s - 8)
            q_arrived(c)
            b_copy(c).start()

        @pl.when(s == 5)
        def _():
            compute_shared()

        if near > 1:

            @pl.when(s == 7)
            def _():
                for c in range(1, near):
                    near_z(c).wait_recv()
                    z_copy(c).wait_recv()
                    p_own(c).start()
                    near_p_own(c).start()
                    for i in range(1, plane):
                        p_copy(c, i).start()
                        near_p(c, i).start()

        @pl.when(s == 8)
        def _():
            arrived(kv_all.at[:, 0], a_recv.at[3])
            ask_far.wait_recv()

        @pl.when((s >= 8) & (s < 11))
        def _():
            first = (s - 8) * share
            lax.fori_loop(first, jnp.minimum(first + share, turns), attend_turn, 0)

        @pl.when(s == 10)
        def _():
            finish_attention()
            answer_far.start()

        @pl.when(s == 9)
        def _():
            arrived(near_return.at[0, others], n_recv.at[6])
            near_q_own(0).wait()
            combine_near()
            for way in range(2):
                shared_copy(2, way).start()

        @pl.when(s == 11)
        def _():
            shared_arrived(2)
            for way in range(2):
                part = pl.ds(way * shared_half, shared_half)
                shared_part[2 - way, part] = (
                    shared_part[2 - way, part].astype(f32) + shared_first[way].astype(f32)
                ).astype(bf16)
                shared_copy(3, way).start()

        @pl.when(s == 12)
        def _():
            answer_far.wait_recv()
            answer_own.start()
            for i in range(1, lines):
                answer_copy(i).start()

        @pl.when(s == 13)
        def _():
            arrived(attended.at[outer], a_recv.at[2])
            answer_own.wait()
            mix()
            for way in range(2):
                mixer_copy(0, way).start()

        return unused

    lax.fori_loop(0, max(summed + 8, 14), step, 0)

    shared_arrived(4)
    for way in range(2):
        part = pl.ds(way * mixer_half, mixer_half)
        mixer_part[side[way], part] = (
            mixer_part[side[way], part].astype(f32) + mixer_first[way].astype(f32)
        ).astype(bf16)
        mixer_copy(1, way).start()
    arrived(back, b_recv.at[0])
    rows_back = back[...].reshape(summed * block_slots, width)
    combined = sum(
        lax.dot_general(m[...], rows_back, (((0,), (0,)), ((), ())), preferred_element_type=f32)
        for m in (mixing_high, mixing_low)
    )
    shared_arrived(3)
    combined = (
        combined
        + shared_part[0].astype(f32)
        + shared_second[0].astype(f32)
        + shared_second[1].astype(f32)
    )
    expert_out[...] = root_norm(combined, exit_gain_ref[...]).astype(bf16)

    shared_arrived(5)
    mixer_out[...] = root_norm(
        mixer_part[own_x].astype(f32) + mixer_second[0].astype(f32) + mixer_second[1].astype(f32),
        mixer_gain_ref[...],
    ).astype(bf16)
    for ref, sem in (
        (stage.at[pl.ds(0, groups - 1)], z_send.at[0]),
        (stage.at[:, others], p_send.at[0]),
        (rows.at[pl.ds(0, 2), pl.ds(0, far)], x_send.at[0]),
        (rows.at[0, pl.ds(0, far)], x_send.at[1]),
        (partial.at[0, pl.ds(0, summed)], x_send.at[2]),
        (partial.at[pl.ds(0, 2), pl.ds(0, summed)], x_send.at[3]),
        (returned.at[pl.ds(0, summed), others], q_send.at[0]),
        (returned.at[pl.ds(0, summed)], b_send.at[0]),
        (meta.at[pl.ds(1, 3)], m_send.at[0]),
        (kv_all.at[own_z, own_core, outer], a_send.at[0]),
        (queries.at[outer], a_send.at[1]),
        (attended.at[outer], a_send.at[2]),
        (kv_all.at[:, 0], a_send.at[3]),
        (kv_all.at[pl.ds(0, groups - 1), 0], a_send.at[6]),
        (near_out.at[:, others], n_send.at[1]),
        (near_return.at[0, others], n_send.at[2]),
    ):
        left_here(ref, sem)
    if near > 1:
        left_here(near_stage.at[pl.ds(0, near - 1)], n_send.at[0])
    for kind, ref in enumerate(shared_landing):
        left_here(ref, s_send.at[kind])
    ask_far.wait_send()
    answer_far.wait_send()


def on_device(
    query_rows,
    key_rows,
    value_rows,
    key_bias,
    mixer_weight,
    mixer_gain,
    routed_input,
    entry_gain,
    expert_index,
    route_weights,
    expert_gate,
    expert_up,
    expert_down,
    shared_gate,
    shared_up,
    shared_down,
    exit_gain,
):
    bf16, f32 = jnp.bfloat16, jnp.float32
    plane = PLANE
    groups = lax.axis_size("ep") // plane
    lines, half = plane // 2, plane // 2
    tokens = query_rows.shape[0]
    count, width = routed_input.shape
    experts = expert_gate.shape[0]
    block = (plane, experts, CAPACITY, width)
    near = min(NEAR, groups)
    kept_slots = (groups - 1) * plane * experts * CAPACITY
    vmem = pl.BlockSpec(memory_space=pltpu.VMEM)
    hbm = pl.BlockSpec(memory_space=pl.ANY)
    weights = (expert_gate, expert_up, expert_down, shared_gate, shared_up, shared_down)
    dma = pltpu.SemaphoreType.DMA
    return pl.pallas_call(
        functools.partial(program_kernel, groups, plane),
        out_shape=(
            jax.ShapeDtypeStruct((tokens // 4, width), bf16),
            jax.ShapeDtypeStruct((count, width), bf16),
        ),
        in_specs=[vmem] * 4 + [hbm] + [vmem] * 6 + [hbm] * 6,
        out_specs=(vmem, vmem),
        scratch_shapes=[
            pltpu.VMEM((count, width), bf16),
            pltpu.VMEM((groups,) + block, bf16),
            pltpu.VMEM((groups - 1,) + block, bf16),
            pltpu.VMEM((groups,) + block, bf16),
            pltpu.VMEM((4, groups) + block, bf16),
            pltpu.VMEM((4, groups) + block, bf16),
            pltpu.VMEM((2, groups, half) + block[1:], bf16),
            pltpu.VMEM((2, groups) + block, bf16),
            pltpu.VMEM((groups,) + block, bf16),
            pltpu.VMEM((groups,) + block, bf16),
            pltpu.VMEM((3, count, width), bf16),
            pltpu.VMEM((4, count, width), bf16),
            pltpu.VMEM((2, count // 2, width), bf16),
            pltpu.VMEM((2, count, width), bf16),
            pltpu.VMEM((lines, tokens + 16, 128), bf16),
            pltpu.VMEM((lines, tokens, 128), bf16),
            pltpu.VMEM((groups, 2, lines, tokens + 16, 128), bf16),
            pltpu.VMEM((6, tokens, 128), bf16),
            pltpu.VMEM((2, 2 * tokens, 128), f32),
            pltpu.VMEM((2, 2 * tokens, 128), f32),
            pltpu.VMEM((2, tokens, 128), bf16),
            pltpu.VMEM((lines, tokens, 128), bf16),
            pltpu.VMEM((lines, tokens, 128), bf16),
            pltpu.VMEM((4, tokens // 4, width), bf16),
            pltpu.VMEM((2, tokens // 8, width), bf16),
            pltpu.VMEM((2, tokens // 4, width), bf16),
            pltpu.VMEM(mixer_weight.shape, bf16),
        ]
        + [pltpu.VMEM(w.shape, bf16) for w in weights]
        + [
            pltpu.VMEM((kept_slots, count), bf16),
            pltpu.VMEM((kept_slots, count), bf16),
            pltpu.VMEM((2 * tokens, 2 * tokens), bf16),
            pltpu.VMEM((4, 8, 128), f32),
            pltpu.VMEM((near, plane, 3) + block[1:], bf16),
            pltpu.VMEM((max(near - 1, 1), plane, 3) + block[1:], bf16),
            pltpu.VMEM((1, plane, 4) + block[1:], bf16),
            dma((7,)),
            dma((2 * groups + 8,)),
            dma((1,)),
            dma((groups,)),
            dma((1,)),
            dma((groups,)),
            dma((4,)),
            dma((4, groups)),
            dma((1,)),
            dma((groups,)),
            dma((1,)),
            dma((1,)),
            dma((6,)),
            dma((6,)),
            dma((7,)),
            dma((6 + groups,)),
            dma((3,)),
            dma((7,)),
            dma((1,)),
            dma((2,)),
        ],
        compiler_params=pltpu.CompilerParams(
            collective_id=1, has_side_effects=True, vmem_limit_bytes=62 << 20
        ),
        name="program",
    )(
        query_rows,
        key_rows,
        value_rows,
        jnp.transpose(key_bias),
        mixer_weight,
        mixer_gain.reshape(1, width),
        routed_input,
        entry_gain.reshape(1, width),
        jnp.transpose(expert_index),
        jnp.transpose(route_weights),
        exit_gain.reshape(1, width),
        *weights,
    )


def solution(mesh):
    in_specs = (
        P("ep", "tp"),
        P("ep", "tp"),
        P("ep", "tp"),
        P("ep", "tp"),
        P("tp", None),
        P(),
        P(("ep", "tp"), None),
        P(),
        P(("ep", "tp"), None),
        P(("ep", "tp"), None),
        P("ep", None, "tp"),
        P("ep", None, "tp"),
        P("ep", "tp", None),
        P(None, "tp"),
        P(None, "tp"),
        P("tp", None),
        P(),
    )
    out_specs = (P(("ep", "tp"), None), P(("ep", "tp"), None))
    return jax.shard_map(
        on_device, mesh=mesh, in_specs=in_specs, out_specs=out_specs, check_vma=False
    )
```
